256 devices in a mesh: sp: 16 (over y, x), dp: 16 (over z, core).
Axes of the slice: x: 4, y: 4, z: 8, core: 2. Of those that a mesh axis runs over, the one named last changes fastest.
Arguments:
- tokens: bfloat16 [16, 4096, 2048], P('dp', 'sp'), may hold values from -200 to 200
- w_qdown: bfloat16 [2048, 512], P('dp'), may hold values from -0.125 to 0.125
- w_kvdown: bfloat16 [2048, 512], P('dp'), may hold values from -0.125 to 0.125
- w_rotary: bfloat16 [2048, 64], replicated, may hold values from -0.125 to 0.125
- q_gain: float32 [512], replicated, may hold values from 0.1 to 1.9
- kv_gain: float32 [512], replicated, may hold values from 0.1 to 1.9
- w_qup: bfloat16 [512, 3072], P('dp'), may hold values from -1 to 1
- w_kvup: bfloat16 [512, 4096], P('dp'), may hold values from -1 to 1
- w_out: bfloat16 [2048, 2048], P(None, 'dp'), may hold values from -0.125 to 0.125
- out_gain: float32 [2048], replicated, may hold values from 0.1 to 1.9
Outputs:
- mixed: bfloat16 [16, 4096, 2048], P('dp', 'sp')
The draws below stay inside these ranges and needn't reach their ends.
All inputs are finite; a program needn't handle non-finite values.
Results may differ from the reference program's by a relative error of at most 0.01.
The reference program's roundings to bfloat16 on the way count: a program that leaves them out, or rounds other values in their place, can miss the bound.
Values may be sent and summed in bfloat16 or wider, within the bound.
No kernel may reach another device: no remote copies, remote signals or barrier semaphores. Data moves between devices by JAX's collectives and lax.ppermute only.
A program may use at most 128 MiB of HBM per device.

```python
import math
import jax
import jax.numpy as jnp
from jax import lax

D = 2048
HEADS = 16
Q_RANK = 512
KV_RANK = 512
NOPE = 128
ROPE = 64
VDIM = 128
LENGTH = 4096
BATCH = 16


def draw_tokens(key, part):
    value_key = jax.random.fold_in(key, 11)
    values = jnp.clip(jax.random.normal(value_key, (BATCH, LENGTH, D), jnp.float32), -6.0, 6.0)
    return values.astype(jnp.bfloat16)


def base_weight(key, salt, rank, width):
    normal = jax.random.normal(jax.random.fold_in(key, salt), (rank, HEADS, width), jnp.float32)
    return jnp.clip(normal, -4.0, 4.0) * rank ** (-0.5)


def draw_w_qup(key, part):
    values = base_weight(key, 41, Q_RANK, NOPE + ROPE)
    values = jnp.clip(values, -1.0, 1.0)
    return values.reshape(Q_RANK, HEADS * (NOPE + ROPE)).astype(jnp.bfloat16)


def draw_w_kvup(key, part):
    values = base_weight(key, 51, KV_RANK, NOPE + VDIM)
    values = jnp.clip(values, -1.0, 1.0)
    return values.reshape(KV_RANK, HEADS * (NOPE + VDIM)).astype(jnp.bfloat16)


def levels(rng, extent, split, least, largest):
    def one(axis_at, blocks):
        draws = jax.random.uniform(jax.random.fold_in(jax.random.fold_in(rng, 6), axis_at), (blocks,), jnp.float32, least / len(split), largest / len(split))
        return jnp.repeat(jnp.exp(draws), extent[axis_at] // blocks).reshape((-1,) + (1,) * (len(extent) - axis_at - 1))

    level = one(*split[0])
    for cut in split[1:]:
        level = level * one(*cut)
    return level


def centred(stream_key, extent, scale, reach, cuts=(), dtype=jnp.bfloat16):
    factor_of = levels(stream_key, extent, cuts, -0.22, 0.18) if cuts else 1.0
    result = jax.random.normal(stream_key, extent, jnp.float32) * scale * factor_of
    return jnp.minimum(jnp.maximum(result, -reach), reach).astype(dtype)


def setup_inputs(seed: int = 0) -> dict:
    arg_keys = jax.random.split(jax.random.key(seed), 11)
    return {
        "tokens": draw_tokens(jax.random.fold_in(arg_keys[10], 71), 0),
        "w_qdown": centred(arg_keys[1], (D, Q_RANK), D ** -0.5, 0.125, ((0, 16),)),
        "w_kvdown": centred(arg_keys[2], (D, KV_RANK), D ** -0.5, 0.125, ((0, 16),)),
        "w_rotary": centred(arg_keys[3], (D, ROPE), D ** -0.5, 0.125),
        "q_gain": jnp.clip(1.0 + 0.18 * jax.random.normal(arg_keys[4], (Q_RANK,), jnp.float32), 0.1, 1.9),
        "kv_gain": jnp.clip(1.0 + 0.18 * jax.random.normal(arg_keys[5], (KV_RANK,), jnp.float32), 0.1, 1.9),
        "w_qup": draw_w_qup(jax.random.fold_in(arg_keys[10], 71), 0),
        "w_kvup": draw_w_kvup(jax.random.fold_in(arg_keys[10], 71), 0),
        "w_out": centred(arg_keys[8], (HEADS * VDIM, D), (HEADS * VDIM) ** -0.5, 0.125, ((1, 16),)),
        "out_gain": jnp.clip(1.0 + 0.18 * jax.random.normal(arg_keys[9], (D,), jnp.float32), 0.1, 1.9),
    }


EPSILON = 1e-06
THETA = 10000.0

def norm_rows(values, gain):
    scale = lax.rsqrt(lax.optimization_barrier(jnp.mean(values * values, axis=-1, keepdims=True)) + EPSILON)
    return values * scale * gain

def rotate(values, cosine, sine):
    half = values.shape[-1] // 2
    first = values[..., :half]
    second = values[..., half:]
    return jnp.concatenate([first * cosine - second * sine, second * cosine + first * sine], axis=-1)

def reference(tokens, w_qdown, w_kvdown, w_rotary, q_gain, kv_gain, w_qup, w_kvup, w_out, out_gain):
    length = tokens.shape[1]
    positions = jnp.arange(length).astype(jnp.float32)
    freqs = THETA ** (-jnp.arange(0, ROPE, 2).astype(jnp.float32) / ROPE)
    angles = positions[:, None] * freqs[None, :]
    cosine = jnp.cos(angles)
    sine = jnp.sin(angles)
    block = math.gcd(length, 512)
    qk_width = NOPE + ROPE
    scaling = qk_width ** (-0.5)

    def one_sequence(sequence):
        q_lat = jnp.dot(sequence, w_qdown, preferred_element_type=jnp.float32)
        kv_lat = jnp.dot(sequence, w_kvdown, preferred_element_type=jnp.float32)
        q_norm = norm_rows(q_lat, q_gain).astype(jnp.bfloat16)
        kv_norm = norm_rows(kv_lat, kv_gain).astype(jnp.bfloat16)
        key_rot = rotate(jnp.dot(sequence, w_rotary, preferred_element_type=jnp.float32), cosine, sine).astype(jnp.bfloat16)
        q_full = jnp.dot(q_norm, w_qup, preferred_element_type=jnp.float32).reshape(length, HEADS, qk_width)
        q_turn = rotate(q_full[..., NOPE:], cosine[:, None, :], sine[:, None, :])
        queries = jnp.concatenate([q_full[..., :NOPE], q_turn], axis=-1).astype(jnp.bfloat16)
        keyval = jnp.dot(kv_norm, w_kvup, preferred_element_type=jnp.float32).astype(jnp.bfloat16)
        keyval = keyval.reshape(length, HEADS, NOPE + VDIM)
        keys_all = keyval[..., :NOPE].astype(jnp.float32)
        values_all = keyval[..., NOPE:].astype(jnp.float32)
        rot_all = key_rot.astype(jnp.float32)
        outputs = []
        for begin in range(0, length, block):
            finish = begin + block
            query_block = queries[begin:finish].astype(jnp.float32)
            scores = jnp.einsum('qhd,khd->hqk', query_block[..., :NOPE], keys_all[:finish])
            scores = scores + jnp.einsum('qhd,kd->hqk', query_block[..., NOPE:], rot_all[:finish])
            scores = scores * scaling
            query_pos = begin + jnp.arange(block)
            key_pos = jnp.arange(finish)
            allowed = key_pos[None, :] <= query_pos[:, None]
            scores = jnp.where(allowed[None], scores, -jnp.inf)
            top = lax.optimization_barrier(jnp.max(scores, axis=-1, keepdims=True))
            expo = jnp.exp(scores - top)
            weights = (expo / lax.optimization_barrier(jnp.sum(expo, axis=-1, keepdims=True))).astype(jnp.bfloat16)
            attended = jnp.einsum('hqk,khd->qhd', weights.astype(jnp.float32), values_all[:finish])
            outputs.append(attended.astype(jnp.bfloat16))
        attended_all = jnp.concatenate(outputs, axis=0).reshape(length, HEADS * VDIM)
        proj = jnp.dot(attended_all, w_out, preferred_element_type=jnp.float32)
        return norm_rows(proj, out_gain).astype(jnp.bfloat16)
    return lax.map(one_sequence, tokens)
```

```python
import jax
import jax.numpy as jnp
from jax import lax
from jax.experimental import pallas as pl
from jax.experimental.pallas import tpu as pltpu
from jax.sharding import PartitionSpec as P

HEADS = 16
NOPE = 128
ROPE = 64
VDIM = 128
RANK = 512
ROWS = 256
SIDE = 4
LENGTH = 4096
LOCAL = HEADS // SIDE
PIECE = 144

EPSILON = 1e-06
THETA = 10000.0
LOG2E = 1.4426950408889634
SCALE2 = (NOPE + ROPE) ** (-0.5) * LOG2E
MIB = 2**20


f32 = jnp.float32
bf16 = jnp.bfloat16


def z_shift(k):
    return [(d, (d + 2 * k) % 16) for d in range(16)]


PARTNER = [(d, d ^ 1) for d in range(16)]


def y_shift(k):
    return [(s, (s + SIDE * k) % 16) for s in range(16)]


def x_shift(k):
    return [(s, (s // SIDE) * SIDE + (s % SIDE + k) % SIDE) for s in range(16)]


def z_blocks(w, up):
    blocks = [w] + [None] * 7
    ahead = behind = w
    for i in range(1, 4):
        ahead = lax.ppermute(ahead, "dp", z_shift(1))
        behind = lax.ppermute(behind, "dp", z_shift(-1))
        blocks[i] = ahead
        blocks[8 - i] = behind
    blocks[4] = lax.ppermute(ahead if up else behind, "dp", z_shift(1 if up else -1))
    return blocks


def call(kernel, out_shape, **kw):
    return pl.pallas_call(
        kernel,
        out_shape=out_shape,
        compiler_params=pltpu.CompilerParams(vmem_limit_bytes=56 * MIB),
        **kw,
    )


SMEM = pl.BlockSpec(memory_space=pltpu.SMEM)
VMEM = pl.BlockSpec(memory_space=pltpu.VMEM)


def down_kernel(z_ref, mine_ref, theirs_ref, *refs):
    blocks, (own_ref, other_ref, w_ref) = refs[:8], refs[8:]
    z = z_ref[0]
    for i, block in enumerate(blocks):
        at = pl.multiple_of(((z - i + 8) % 8) * 128, 128)
        w_ref[pl.ds(at, 128), :] = block[...]
    w = w_ref[...]
    own_ref[...] = jnp.dot(mine_ref[...], w, preferred_element_type=f32)
    other_ref[...] = jnp.dot(theirs_ref[...], w, preferred_element_type=f32)


def down(z, mine, theirs, blocks):
    part = jax.ShapeDtypeStruct((ROWS, RANK), f32)
    return call(
        down_kernel,
        (part, part),
        in_specs=[SMEM] + [VMEM] * 10,
        out_specs=(VMEM, VMEM),
        scratch_shapes=[pltpu.VMEM((1024, RANK), bf16)],
        name="down",
    )(z, mine, theirs, *blocks)


def normed(values, gain):
    scale = lax.rsqrt(jnp.mean(values * values, axis=-1, keepdims=True) + EPSILON)
    return values * scale * gain


def kv_norm_kernel(own_ref, recv_ref, gain_ref, rot_ref, a_ref, b_ref):
    kvn = normed(own_ref[...] + recv_ref[...], gain_ref[...]).astype(bf16)
    a_ref[0:128, :] = kvn[0:128]
    a_ref[128:PIECE, :] = rot_ref[0]
    b_ref[0:128, :] = kvn[128:256]
    b_ref[128:PIECE, :] = rot_ref[1]


def q_norm_kernel(own_ref, recv_ref, gain_ref, q_ref):
    q_ref[...] = normed(own_ref[...] + recv_ref[...], gain_ref[...]).astype(bf16)


def up_kernel(
    yx_ref, a0, a1, a2l, a2h, a3, b0, b1, b2l, b2h, b3, w_ref, cos_ref, sin_ref,
    k_ref, r_ref, vt_ref, q_ref, wvt_ref,
):
    y = yx_ref[0]
    x = yx_ref[1]
    wvt_ref[...] = w_ref[:, 512:1024].T

    def reader(low, high=None):
        def read(at, count):
            if high is None:
                return low[at : at + count, :]
            cut = low.shape[0]
            if at < cut:
                return low[at : at + count, :]
            return high[at - cut : at - cut + count, :]

        return read

    def expand(read, spots):
        rows = jnp.concatenate([read(PIECE * n, 128) for n in range(4)], axis=0)
        keys = jnp.dot(rows, w_ref[:, 0:512], preferred_element_type=f32).astype(bf16)
        values = lax.dot_general(
            wvt_ref[...], rows, (((1,), (1,)), ((), ())), preferred_element_type=f32
        ).astype(bf16)
        for n in range(4):
            at = pl.multiple_of(spots[n], 128)
            k_ref[pl.ds(at, 128), :] = keys[128 * n : 128 * n + 128]
            vt_ref[:, pl.ds(at, 128)] = values[:, 128 * n : 128 * n + 128]
            packed = read(PIECE * n + 128, 16)
            rot = jnp.concatenate([packed[:, 64 * u : 64 * u + 64] for u in range(8)], axis=0)
            r_ref[pl.ds(at, 128), :] = jnp.concatenate([rot, jnp.zeros((128, 64), bf16)], axis=1)

    def spot(i, j, half):
        return ((y - i + 4) % 4 * 4 + (x - j + 4) % 4) * 256 + half * 128

    for j, read in enumerate([reader(a0), reader(a1), reader(a2l, a2h), reader(a3)]):
        expand(read, [spot(i, j, 0) for i in range(4)])
    for i, read in enumerate([reader(b0), reader(b1), reader(b2l, b2h), reader(b3)]):
        expand(read, [spot(i, j, 1) for j in range(4)])
        qn = read(4 * PIECE, ROWS)
        both = jnp.dot(qn, w_ref[:, 1024:2048], preferred_element_type=f32)
        cosine = jnp.concatenate([cos_ref[i], cos_ref[i]], axis=1)
        sine = jnp.concatenate([sin_ref[i], sin_ref[i]], axis=1)
        turned = (both[:, 512:768] * cosine + both[:, 768:1024] * sine).astype(bf16)
        pad = jnp.zeros((ROWS, 64), bf16)
        for h in range(LOCAL):
            q_ref[h, ROWS * i : ROWS * (i + 1), 0:128] = both[:, 128 * h : 128 * h + 128].astype(bf16)
            q_ref[h, ROWS * i : ROWS * (i + 1), 128:256] = jnp.concatenate(
                [turned[:, 64 * h : 64 * h + 64], pad], axis=1
            )


def expand_all(yx, parts, w_up, cosine, sine):
    out = (
        jax.ShapeDtypeStruct((LENGTH, LOCAL * 128), bf16),
        jax.ShapeDtypeStruct((LENGTH, 128), bf16),
        jax.ShapeDtypeStruct((LOCAL * 128, LENGTH), bf16),
        jax.ShapeDtypeStruct((LOCAL, SIDE * ROWS, 256), bf16),
    )
    return call(
        up_kernel,
        out,
        in_specs=[SMEM] + [VMEM] * 13,
        out_specs=(VMEM,) * 4,
        scratch_shapes=[pltpu.VMEM((512, 512), bf16)],
        name="expand",
    )(yx, *parts, w_up, cosine, sine)


KEYS = 512
PAIR = 2


def attend_kernel(s_ref, q_ref, k_ref, r_ref, vt_ref, o_ref, score_ref, top_ref, sum_ref, acc_ref):
    s = s_ref[pl.program_id(1)]

    def score(at, slot, ahead):
        rot = r_ref[pl.ds(at, KEYS), :]
        for h in range(PAIR):
            keys = jnp.concatenate([k_ref[pl.ds(at, KEYS), 128 * h : 128 * h + 128], rot], axis=1)
            st = lax.dot_general(keys, q_ref[h], (((1,), (1,)), ((), ())), preferred_element_type=f32)
            if ahead is not None:
                key_pos = lax.broadcasted_iota(jnp.int32, st.shape, 0)
                query_pos = lax.broadcasted_iota(jnp.int32, st.shape, 1)
                st = jnp.where(key_pos <= query_pos + ahead, st, -jnp.inf)
            score_ref[slot, h] = st

    def add(at, slot):
        for h in range(PAIR):
            st = score_ref[slot, h]
            top = top_ref[h]
            new = jnp.maximum(top, jnp.max(st, axis=0, keepdims=True))
            expo = jnp.exp2(st * SCALE2 - new * SCALE2)
            fade = jnp.exp2((top - new) * SCALE2)
            top_ref[h] = new
            sum_ref[h] = sum_ref[h] * fade + jnp.sum(expo, axis=0, keepdims=True)
            acc_ref[h] = acc_ref[h] * fade + jnp.dot(
                vt_ref[128 * h : 128 * h + 128, pl.ds(at, KEYS)], expo.astype(bf16), preferred_element_type=f32
            )

    top_ref[...] = jnp.full(top_ref.shape, -jnp.inf, f32)
    sum_ref[...] = jnp.zeros(sum_ref.shape, f32)
    acc_ref[...] = jnp.zeros(acc_ref.shape, f32)
    full = s // 2
    last = pl.multiple_of(full * KEYS, KEYS)

    def at(j):
        return pl.multiple_of(j * KEYS, KEYS)

    def before(j):
        return pl.multiple_of(jnp.where(j == 0, full, j - 1) * KEYS, KEYS)

    score(last, 0, s * ROWS - last)

    def body(t, carry):
        j = 2 * t
        score(at(j), 1, None)
        add(before(j), 0)
        score(at(j + 1), 0, None)
        add(at(j), 1)
        return carry

    lax.fori_loop(0, full // 2, body, 0)

    @pl.when(full % 2 == 1)
    def _():
        score(at(full - 1), 1, None)
        add(before(full - 1), 0)
        add(at(full - 1), 1)

    @pl.when(full % 2 == 0)
    def _():
        add(before(full), 0)

    for h in range(PAIR):
        o_ref[0, h * 128 : (h + 1) * 128, :] = (acc_ref[h] / sum_ref[h]).astype(bf16)


def attend(spots, queries, keys, rot, values):
    grid_spec = pltpu.PrefetchScalarGridSpec(
        num_scalar_prefetch=1,
        grid=(LOCAL // PAIR, SIDE),
        in_specs=[
            pl.BlockSpec((PAIR, ROWS, 256), lambda h, i, s: (h, i, 0)),
            pl.BlockSpec((LENGTH, PAIR * 128), lambda h, i, s: (0, h)),
            pl.BlockSpec((LENGTH, 128), lambda h, i, s: (0, 0)),
            pl.BlockSpec((PAIR * 128, LENGTH), lambda h, i, s: (h, 0)),
        ],
        out_specs=pl.BlockSpec((1, PAIR * 128, ROWS), lambda h, i, s: (i, h, 0)),
        scratch_shapes=[
            pltpu.VMEM((2, PAIR, KEYS, ROWS), f32),
            pltpu.VMEM((PAIR, 1, ROWS), f32),
            pltpu.VMEM((PAIR, 1, ROWS), f32),
            pltpu.VMEM((PAIR, 128, ROWS), f32),
        ],
    )
    return pl.pallas_call(
        attend_kernel,
        grid_spec=grid_spec,
        out_shape=jax.ShapeDtypeStruct((SIDE, LOCAL * 128, ROWS), bf16),
        compiler_params=pltpu.CompilerParams(
            dimension_semantics=("arbitrary", "arbitrary"), vmem_limit_bytes=56 * MIB
        ),
        name="attend",
    )(spots, queries, keys, rot, values)


WIDE = 512


def out_kernel(y_ref, p0, p1, p2, p3, w_ref, gain_ref, o_ref, rows_ref, proj_ref):
    n = pl.program_id(0)
    y = y_ref[0]

    @pl.when(n == 0)
    def _():
        for i, piece in enumerate((p0, p1, p2, p3)):
            g = pl.multiple_of(((y + i) % 4) * 512, 512)
            rows_ref[:, pl.ds(g, 512)] = piece[...].T

    proj_ref[:, pl.ds(pl.multiple_of(n * WIDE, WIDE), WIDE)] = jnp.dot(
        rows_ref[...], w_ref[...], preferred_element_type=f32
    )

    @pl.when(n == pl.num_programs(0) - 1)
    def _():
        o_ref[...] = normed(proj_ref[...], gain_ref[...]).astype(bf16)


def project(y, pieces, w_out, gain):
    return pl.pallas_call(
        out_kernel,
        grid=(2048 // WIDE,),
        in_specs=[SMEM]
        + [pl.BlockSpec((512, ROWS), lambda n: (0, 0))] * 4
        + [
            pl.BlockSpec((2048, WIDE), lambda n: (0, n)),
            pl.BlockSpec((1, 2048), lambda n: (0, 0)),
        ],
        out_specs=pl.BlockSpec((ROWS, 2048), lambda n: (0, 0)),
        out_shape=jax.ShapeDtypeStruct((ROWS, 2048), bf16),
        scratch_shapes=[pltpu.VMEM((ROWS, 2048), bf16), pltpu.VMEM((ROWS, 2048), f32)],
        compiler_params=pltpu.CompilerParams(
            dimension_semantics=("arbitrary",), vmem_limit_bytes=56 * MIB
        ),
        name="project",
    )(y, *pieces, w_out, gain)


def up_columns(w_qup, w_kvup, y):
    rows = w_qup.shape[0]
    q = lax.dynamic_slice_in_dim(w_qup, y * LOCAL * 192, LOCAL * 192, 1).reshape(rows, LOCAL, 192)
    kv = lax.dynamic_slice_in_dim(w_kvup, y * LOCAL * 256, LOCAL * 256, 1).reshape(rows, LOCAL, 256)
    first = q[..., 128:160]
    second = q[..., 160:192]
    parts = [
        kv[..., :128],
        kv[..., 128:],
        q[..., :128],
        jnp.concatenate([first, second], axis=-1),
        jnp.concatenate([-second, first], axis=-1),
    ]
    return jnp.concatenate([p.reshape(rows, -1) for p in parts], axis=1)


def body(tokens, w_qdown, w_kvdown, w_rotary, q_gain, kv_gain, w_qup, w_kvup, w_out, out_gain):
    dp_place = lax.axis_index("dp")
    sp_place = lax.axis_index("sp")
    z = (dp_place // 2).reshape(1)
    core = dp_place % 2
    y = sp_place // SIDE
    x = sp_place % SIDE
    own = tokens[0]

    halves = own.reshape(ROWS, 8, 2, 128)
    mine = jnp.where(core == 0, halves[:, :, 0], halves[:, :, 1]).reshape(ROWS, 1024)
    other = jnp.where(core == 0, halves[:, :, 1], halves[:, :, 0]).reshape(ROWS, 1024)
    theirs = lax.ppermute(other, "dp", PARTNER)
    kv_blocks = z_blocks(w_kvdown, True)
    q_blocks = z_blocks(w_qdown, False)

    spots = ((y - jnp.arange(SIDE) + SIDE) % SIDE) * SIDE + x
    positions = (spots[:, None] * ROWS + jnp.arange(ROWS)[None, :]).astype(f32)
    freqs = THETA ** (-jnp.arange(0, ROPE, 2).astype(f32) / ROPE)
    angles = positions[..., None] * freqs
    cosine = jnp.cos(angles)
    sine = jnp.sin(angles)
    cos_wide = jnp.concatenate([cosine] * 4, axis=-1)
    sin_wide = jnp.concatenate([sine] * 4, axis=-1)

    turned = jnp.dot(own, w_rotary, preferred_element_type=f32)
    first = turned[:, :32]
    second = turned[:, 32:]
    key_rot = jnp.concatenate(
        [first * cosine[0] - second * sine[0], second * cosine[0] + first * sine[0]], axis=-1
    ).astype(bf16)
    packed = key_rot.reshape(2, 8, 16, 64).transpose(0, 2, 1, 3).reshape(2, 16, 512)

    w_up = lax.all_gather(up_columns(w_qup, w_kvup, y), "dp", axis=0, tiled=True)
    w_full = lax.all_gather(w_out, "dp", axis=1, tiled=True)

    kv_own, kv_other = down(z, mine, theirs, kv_blocks)
    kv_recv = lax.ppermute(kv_other, "dp", PARTNER)
    piece = jax.ShapeDtypeStruct((PIECE, RANK), bf16)
    a, b = call(kv_norm_kernel, (piece, piece), name="kvnorm")(
        kv_own, kv_recv, kv_gain.reshape(1, RANK), packed
    )

    q_own, q_other = down(z, mine, theirs, q_blocks)
    q_recv = lax.ppermute(q_other, "dp", PARTNER)
    qn = call(q_norm_kernel, jax.ShapeDtypeStruct((ROWS, RANK), bf16), name="qnorm")(
        q_own, q_recv, q_gain.reshape(1, RANK)
    )

    a1 = lax.ppermute(a, "sp", y_shift(1))
    a3 = lax.ppermute(a, "sp", y_shift(-1))
    b1 = lax.ppermute(b, "sp", x_shift(1))
    b3 = lax.ppermute(b, "sp", x_shift(-1))
    a2 = lax.ppermute(a1, "sp", y_shift(1))
    b2 = lax.ppermute(b3, "sp", x_shift(-1))
    col = jnp.concatenate([a, a1, a2, a3], axis=0)
    row = jnp.concatenate([b, b1, b2, b3, qn], axis=0)
    col1 = lax.ppermute(col, "sp", x_shift(1))
    col3 = lax.ppermute(col, "sp", x_shift(-1))
    row1 = lax.ppermute(row, "sp", y_shift(1))
    row3 = lax.ppermute(row, "sp", y_shift(-1))
    col2l = lax.ppermute(col1[:288], "sp", x_shift(1))
    col2h = lax.ppermute(col3[288:], "sp", x_shift(-1))
    row2l = lax.ppermute(row1[:416], "sp", y_shift(1))
    row2h = lax.ppermute(row3[416:], "sp", y_shift(-1))

    yx = jnp.stack([y, x])
    keys, rot, values, queries = expand_all(
        yx,
        (col, col1, col2l, col2h, col3, row, row1, row2l, row2h, row3),
        w_up,
        cos_wide,
        sin_wide,
    )
    attended = attend(spots, queries, keys, rot, values)
    pieces = [attended[0]] + [
        lax.ppermute(attended[i], "sp", y_shift(-i)) for i in range(1, SIDE)
    ]
    mixed = project(y.reshape(1), pieces, w_full, out_gain.reshape(1, 2048))
    return mixed[None]


def solution(mesh):
    in_specs = (
        P("dp", "sp", None),
        P("dp", None),
        P("dp", None),
        P(),
        P(),
        P(),
        P("dp", None),
        P("dp", None),
        P(None, "dp"),
        P(),
    )
    out_specs = P("dp", "sp", None)
    return jax.shard_map(body, mesh=mesh, in_specs=in_specs, out_specs=out_specs, check_vma=False)
```

```python
import jax
import jax.numpy as jnp
from jax import lax
from jax.experimental import pallas as pl
from jax.experimental.pallas import tpu as pltpu
from jax.sharding import PartitionSpec as P

HEADS = 16
NOPE = 128
ROPE = 64
VDIM = 128
RANK = 512
ROWS = 256
SIDE = 4
LENGTH = 4096
LOCAL = HEADS // SIDE
PIECE = 144

EPSILON = 1e-06
THETA = 10000.0
LOG2E = 1.4426950408889634
SCALE2 = (NOPE + ROPE) ** (-0.5) * LOG2E
MIB = 2**20


f32 = jnp.float32
bf16 = jnp.bfloat16


def y_shift(k):
    return [(s, (s + SIDE * k) % 16) for s in range(16)]


def x_shift(k):
    return [(s, (s // SIDE) * SIDE + (s % SIDE + k) % SIDE) for s in range(16)]


def limit(mib, **kw):
    return pltpu.CompilerParams(vmem_limit_bytes=mib * MIB, **kw)


SMEM = pl.BlockSpec(memory_space=pltpu.SMEM)
VMEM = pl.BlockSpec(memory_space=pltpu.VMEM)


def normed(values, gain):
    scale = lax.rsqrt(jnp.mean(values * values, axis=-1, keepdims=True) + EPSILON)
    return values * scale * gain


def down_kernel(rows_ref, w_ref, gain_ref, rot_ref, a_ref, b_ref, q_ref):
    w = w_ref[...].reshape(2048, RANK)
    lat = jnp.dot(rows_ref[...], w, preferred_element_type=f32)
    lat = normed(lat, gain_ref[0]).astype(bf16)

    @pl.when(pl.program_id(0) == 0)
    def _():
        a_ref[0:128, :] = lat[0:128]
        a_ref[128:PIECE, :] = rot_ref[0]
        b_ref[0:128, :] = lat[128:256]
        b_ref[128:PIECE, :] = rot_ref[1]

    @pl.when(pl.program_id(0) == 1)
    def _():
        q_ref[...] = lat


def down(rows, w, gains, rot):
    piece = jax.ShapeDtypeStruct((PIECE, RANK), bf16)
    return pl.pallas_call(
        down_kernel,
        grid=(2,),
        in_specs=[
            pl.BlockSpec((ROWS, 2048), lambda n: (0, 0)),
            pl.BlockSpec((16, 1, 128, RANK), lambda n: (0, n, 0, 0)),
            pl.BlockSpec((1, 1, RANK), lambda n: (n, 0, 0)),
            pl.BlockSpec((2, 16, RANK), lambda n: (0, 0, 0)),
        ],
        out_specs=(
            pl.BlockSpec((PIECE, RANK), lambda n: (0, 0)),
            pl.BlockSpec((PIECE, RANK), lambda n: (0, 0)),
            pl.BlockSpec((ROWS, RANK), lambda n: (0, 0)),
        ),
        out_shape=(piece, piece, jax.ShapeDtypeStruct((ROWS, RANK), bf16)),
        compiler_params=limit(16, dimension_semantics=("arbitrary",)),
        name="down",
    )(rows, w, gains, rot)


def reader(low, high=None):
    def read(at, count):
        cut = low.shape[0]
        if at < cut:
            return low[at : at + count, :]
        return high[at - cut : at - cut + count, :]

    return read


def spot(yx_ref, i, j, half):
    at = ((yx_ref[0] - i + 4) % 4 * 4 + (yx_ref[1] - j + 4) % 4) * 256 + half * 128
    return pl.multiple_of(at, 128)


def expand(read, spots, w_ref, wvt_ref, k_ref, r_ref, vt_ref):
    rows = jnp.concatenate([read(PIECE * n, 128) for n in range(4)], axis=0)
    keys = jnp.dot(rows, w_ref[:, 0:512], preferred_element_type=f32).astype(bf16)
    values = lax.dot_general(
        wvt_ref[...], rows, (((1,), (1,)), ((), ())), preferred_element_type=f32
    ).astype(bf16)
    for n, at in enumerate(spots):
        for p in range(2):
            k_ref[p, pl.ds(at, 128), :] = keys[128 * n : 128 * n + 128, 256 * p : 256 * p + 256]
            vt_ref[p, :, pl.ds(at, 128)] = values[256 * p : 256 * p + 256, 128 * n : 128 * n + 128]
        packed = read(PIECE * n + 128, 16)
        rot = jnp.concatenate([packed[:, 64 * u : 64 * u + 64] for u in range(8)], axis=0)
        r_ref[pl.ds(at, 128), :] = jnp.concatenate([rot, jnp.zeros((128, 64), bf16)], axis=1)


def expand_queries(qn, i, w_ref, cos_ref, sin_ref, q_ref):
    both = jnp.dot(qn, w_ref[:, 1024:2048], preferred_element_type=f32)
    cosine = jnp.concatenate([cos_ref[i], cos_ref[i]], axis=1)
    sine = jnp.concatenate([sin_ref[i], sin_ref[i]], axis=1)
    turned = (both[:, 512:768] * cosine + both[:, 768:1024] * sine).astype(bf16)
    pad = jnp.zeros((ROWS, 64), bf16)
    for h in range(LOCAL):
        q_ref[h, ROWS * i : ROWS * (i + 1), 0:128] = both[:, 128 * h : 128 * h + 128].astype(bf16)
        q_ref[h, ROWS * i : ROWS * (i + 1), 128:256] = jnp.concatenate(
            [turned[:, 64 * h : 64 * h + 64], pad], axis=1
        )


def early_kernel(
    yx_ref, a0, a1, a3, b0, b1, b3, w_ref, cos_ref, sin_ref, k_ref, r_ref, vt_ref, q_ref, wvt_ref
):
    wvt_ref[...] = w_ref[:, 512:1024].T
    outs = (w_ref, wvt_ref, k_ref, r_ref, vt_ref)
    for j, piece in ((0, a0), (1, a1), (3, a3)):
        expand(reader(piece), [spot(yx_ref, i, j, 0) for i in range(4)], *outs)
    for i, piece in ((0, b0), (1, b1), (3, b3)):
        expand(reader(piece), [spot(yx_ref, i, j, 1) for j in range(4)], *outs)
        expand_queries(piece[4 * PIECE : 4 * PIECE + ROWS, :], i, w_ref, cos_ref, sin_ref, q_ref)


EXPANDED = (
    (2, LENGTH, 256),
    (LENGTH, 128),
    (2, 256, LENGTH),
    (LOCAL, SIDE * ROWS, 256),
)


def expand_early(yx, parts, w_up, cosine, sine):
    return pl.pallas_call(
        early_kernel,
        out_shape=tuple(jax.ShapeDtypeStruct(s, bf16) for s in EXPANDED),
        in_specs=[SMEM] + [VMEM] * 9,
        out_specs=(VMEM,) * 4,
        scratch_shapes=[pltpu.VMEM((512, 512), bf16)],
        compiler_params=limit(24),
        name="early",
    )(yx, *parts, w_up, cosine, sine)


KEYS = 512
PAIR = 2


def attend_kernel(
    yx_ref, a2l, a2h, b2l, b2h, w_ref, cos_ref, sin_ref, k_in, r_in, vt_in, q_in, o_ref,
    k_ref, r_ref, vt_ref, q_ref, wvt_ref, score_ref, top_ref, sum_ref, acc_ref,
):
    pair = pl.program_id(0)
    step = pl.program_id(1)

    @pl.when((pair == 0) & (step == 0))
    def _():
        for p in range(2):
            k_ref[p] = k_in[p]
            vt_ref[p] = vt_in[p]
        r_ref[...] = r_in[...]
        for h in range(LOCAL):
            q_ref[h] = q_in[h]
        wvt_ref[...] = w_ref[:, 512:1024].T
        outs = (w_ref, wvt_ref, k_ref, r_ref, vt_ref)
        expand(reader(a2l, a2h), [spot(yx_ref, i, 2, 0) for i in range(4)], *outs)
        last = reader(b2l, b2h)
        expand(last, [spot(yx_ref, 2, j, 1) for j in range(4)], *outs)
        expand_queries(last(4 * PIECE, ROWS), 2, w_ref, cos_ref, sin_ref, q_ref)

    s = (yx_ref[0] - step + 4) % 4 * 4 + yx_ref[1]
    mine = pl.multiple_of(step * ROWS, ROWS)

    def score(at, slot, ahead):
        rot = r_ref[pl.ds(at, KEYS), :]
        for h in range(PAIR):
            keys = jnp.concatenate([k_ref[pair, pl.ds(at, KEYS), 128 * h : 128 * h + 128], rot], axis=1)
            query = q_ref[PAIR * pair + h, pl.ds(mine, ROWS), :]
            st = lax.dot_general(keys, query, (((1,), (1,)), ((), ())), preferred_element_type=f32)
            if ahead is not None:
                key_pos = lax.broadcasted_iota(jnp.int32, st.shape, 0)
                query_pos = lax.broadcasted_iota(jnp.int32, st.shape, 1)
                st = jnp.where(key_pos <= query_pos + ahead, st, -jnp.inf)
            score_ref[slot, h] = st

    def add(at, slot):
        for h in range(PAIR):
            st = score_ref[slot, h]
            top = top_ref[h]
            new = jnp.maximum(top, jnp.max(st, axis=0, keepdims=True))
            expo = jnp.exp2(st * SCALE2 - new * SCALE2)
            fade = jnp.exp2((top - new) * SCALE2)
            top_ref[h] = new
            sum_ref[h] = sum_ref[h] * fade + jnp.sum(expo, axis=0, keepdims=True)
            acc_ref[h] = acc_ref[h] * fade + jnp.dot(
                vt_ref[pair, 128 * h : 128 * h + 128, pl.ds(at, KEYS)],
                expo.astype(bf16),
                preferred_element_type=f32,
            )

    top_ref[...] = jnp.full(top_ref.shape, -jnp.inf, f32)
    sum_ref[...] = jnp.zeros(sum_ref.shape, f32)
    acc_ref[...] = jnp.zeros(acc_ref.shape, f32)
    full = s // 2
    last = pl.multiple_of(full * KEYS, KEYS)

    def at(j):
        return pl.multiple_of(j * KEYS, KEYS)

    def before(j):
        return pl.multiple_of(jnp.where(j == 0, full, j - 1) * KEYS, KEYS)

    score(last, 0, s * ROWS - last)

    def body(t, carry):
        j = 2 * t
        score(at(j), 1, None)
        add(before(j), 0)
        score(at(j + 1), 0, None)
        add(at(j), 1)
        return carry

    lax.fori_loop(0, full // 2, body, 0)

    @pl.when(full % 2 == 1)
    def _():
        score(at(full - 1), 1, None)
        add(before(full - 1), 0)
        add(at(full - 1), 1)

    @pl.when(full % 2 == 0)
    def _():
        add(before(full), 0)

    for h in range(PAIR):
        o_ref[0, h * 128 : (h + 1) * 128, :] = (acc_ref[h] / sum_ref[h]).astype(bf16)


def attend(yx, halves, w_up, cosine, sine, early):
    return pl.pallas_call(
        attend_kernel,
        grid=(LOCAL // PAIR, SIDE),
        in_specs=[SMEM] + [VMEM] * 11,
        out_specs=pl.BlockSpec((1, PAIR * 128, ROWS), lambda h, i: (i, h, 0)),
        out_shape=jax.ShapeDtypeStruct((SIDE, LOCAL * 128, ROWS), bf16),
        scratch_shapes=[pltpu.VMEM(s, bf16) for s in EXPANDED]
        + [
            pltpu.VMEM((512, 512), bf16),
            pltpu.VMEM((2, PAIR, KEYS, ROWS), f32),
            pltpu.VMEM((PAIR, 1, ROWS), f32),
            pltpu.VMEM((PAIR, 1, ROWS), f32),
            pltpu.VMEM((PAIR, 128, ROWS), f32),
        ],
        compiler_params=limit(32, dimension_semantics=("arbitrary", "arbitrary")),
        name="attend",
    )(yx, *halves, w_up, cosine, sine, *early)


WIDE = 512


def out_kernel(y_ref, p0, p1, p2, p3, w_ref, gain_ref, o_ref, rows_ref, proj_ref):
    n = pl.program_id(0)
    y = y_ref[0]

    @pl.when(n == 0)
    def _():
        for i, piece in enumerate((p0, p1, p2, p3)):
            g = pl.multiple_of(((y + i) % 4) * 512, 512)
            rows_ref[:, pl.ds(g, 512)] = piece[...].T

    proj_ref[:, pl.ds(pl.multiple_of(n * WIDE, WIDE), WIDE)] = jnp.dot(
        rows_ref[...], w_ref[...], preferred_element_type=f32
    )

    @pl.when(n == pl.num_programs(0) - 1)
    def _():
        o_ref[...] = normed(proj_ref[...], gain_ref[...]).astype(bf16)


def project(y, pieces, w_out, gain):
    return pl.pallas_call(
        out_kernel,
        grid=(2048 // WIDE,),
        in_specs=[SMEM]
        + [pl.BlockSpec((512, ROWS), lambda n: (0, 0))] * 4
        + [
            pl.BlockSpec((2048, WIDE), lambda n: (0, n)),
            pl.BlockSpec((1, 2048), lambda n: (0, 0)),
        ],
        out_specs=pl.BlockSpec((ROWS, 2048), lambda n: (0, 0)),
        out_shape=jax.ShapeDtypeStruct((ROWS, 2048), bf16),
        scratch_shapes=[pltpu.VMEM((ROWS, 2048), bf16), pltpu.VMEM((ROWS, 2048), f32)],
        compiler_params=limit(24, dimension_semantics=("arbitrary",)),
        name="project",
    )(y, *pieces, w_out, gain)


def up_columns(w_qup, w_kvup, y):
    rows = w_qup.shape[0]
    q = lax.dynamic_slice_in_dim(w_qup, y * LOCAL * 192, LOCAL * 192, 1).reshape(rows, LOCAL, 192)
    kv = lax.dynamic_slice_in_dim(w_kvup, y * LOCAL * 256, LOCAL * 256, 1).reshape(rows, LOCAL, 256)
    first = q[..., 128:160]
    second = q[..., 160:192]
    parts = [
        kv[..., :128],
        kv[..., 128:],
        q[..., :128],
        jnp.concatenate([first, second], axis=-1),
        jnp.concatenate([-second, first], axis=-1),
    ]
    return jnp.concatenate([p.reshape(rows, -1) for p in parts], axis=1)


def body(tokens, w_qdown, w_kvdown, w_rotary, q_gain, kv_gain, w_qup, w_kvup, w_out, out_gain):
    sp_place = lax.axis_index("sp")
    y = sp_place // SIDE
    x = sp_place % SIDE
    own = tokens[0]
    w_down = lax.all_gather(jnp.stack([w_kvdown, w_qdown]), "dp")

    spots = ((y - jnp.arange(SIDE) + SIDE) % SIDE) * SIDE + x
    positions = (spots[:, None] * ROWS + jnp.arange(ROWS)[None, :]).astype(f32)
    freqs = THETA ** (-jnp.arange(0, ROPE, 2).astype(f32) / ROPE)
    angles = positions[..., None] * freqs
    cosine = jnp.cos(angles)
    sine = jnp.sin(angles)
    cos_wide = jnp.concatenate([cosine] * 4, axis=-1)
    sin_wide = jnp.concatenate([sine] * 4, axis=-1)

    turned = jnp.dot(own, w_rotary, preferred_element_type=f32)
    first = turned[:, :32]
    second = turned[:, 32:]
    key_rot = jnp.concatenate(
        [first * cosine[0] - second * sine[0], second * cosine[0] + first * sine[0]], axis=-1
    ).astype(bf16)
    packed = key_rot.reshape(2, 8, 16, 64).transpose(0, 2, 1, 3).reshape(2, 16, 512)

    w_up = lax.all_gather(up_columns(w_qup, w_kvup, y), "dp", axis=0, tiled=True)
    w_full = lax.all_gather(w_out, "dp", axis=1, tiled=True)

    gains = jnp.stack([kv_gain, q_gain]).reshape(2, 1, RANK)
    a, b, qn = down(own, w_down, gains, packed)

    a1 = lax.ppermute(a, "sp", y_shift(1))
    a3 = lax.ppermute(a, "sp", y_shift(-1))
    b1 = lax.ppermute(b, "sp", x_shift(1))
    b3 = lax.ppermute(b, "sp", x_shift(-1))
    a2 = lax.ppermute(a1, "sp", y_shift(1))
    b2 = lax.ppermute(b3, "sp", x_shift(-1))
    col = jnp.concatenate([a, a1, a2, a3], axis=0)
    row = jnp.concatenate([b, b1, b2, b3, qn], axis=0)
    col1 = lax.ppermute(col, "sp", x_shift(1))
    col3 = lax.ppermute(col, "sp", x_shift(-1))
    row1 = lax.ppermute(row, "sp", y_shift(1))
    row3 = lax.ppermute(row, "sp", y_shift(-1))
    col2l = lax.ppermute(col1[:288], "sp", x_shift(1))
    col2h = lax.ppermute(col3[288:], "sp", x_shift(-1))
    row2l = lax.ppermute(row1[:416], "sp", y_shift(1))
    row2h = lax.ppermute(row3[416:], "sp", y_shift(-1))

    yx = jnp.stack([y, x])
    early = expand_early(yx, (col, col1, col3, row, row1, row3), w_up, cos_wide, sin_wide)
    attended = attend(yx, (col2l, col2h, row2l, row2h), w_up, cos_wide, sin_wide, early)
    pieces = [attended[0]] + [
        lax.ppermute(attended[i], "sp", y_shift(-i)) for i in range(1, SIDE)
    ]
    mixed = project(y.reshape(1), pieces, w_full, out_gain.reshape(1, 2048))
    return mixed[None]


def solution(mesh):
    in_specs = (
        P("dp", "sp", None),
        P("dp", None),
        P("dp", None),
        P(),
        P(),
        P(),
        P("dp", None),
        P("dp", None),
        P(None, "dp"),
        P(),
    )
    out_specs = P("dp", "sp", None)
    return jax.shard_map(body, mesh=mesh, in_specs=in_specs, out_specs=out_specs, check_vma=False)
```

```python
import jax
import jax.numpy as jnp
from jax import lax
from jax.experimental import pallas as pl
from jax.experimental.pallas import tpu as pltpu
from jax.sharding import PartitionSpec as P

HEADS = 16
NOPE = 128
ROPE = 64
VDIM = 128
RANK = 512
ROWS = 256
SIDE = 4
LENGTH = 4096
LOCAL = HEADS // SIDE
PIECE = 144

EPSILON = 1e-06
THETA = 10000.0
LOG2E = 1.4426950408889634
SCALE2 = (NOPE + ROPE) ** (-0.5) * LOG2E
MIB = 2**20


f32 = jnp.float32
bf16 = jnp.bfloat16


PARTNER = [(d, d ^ 1) for d in range(16)]


def z_shift(k):
    return [(d, (d + 2 * k) % 16) for d in range(16)]


def z_blocks(w):
    blocks = [w] + [None] * 7
    ahead = behind = w
    for i in range(1, 4):
        ahead = lax.ppermute(ahead, "dp", z_shift(1))
        behind = lax.ppermute(behind, "dp", z_shift(-1))
        blocks[i] = ahead
        blocks[8 - i] = behind
    blocks[4] = lax.ppermute(ahead, "dp", z_shift(1))
    return jnp.concatenate(blocks, axis=0)


def y_shift(k):
    return [(s, (s + SIDE * k) % 16) for s in range(16)]


def x_shift(k):
    return [(s, (s // SIDE) * SIDE + (s % SIDE + k) % SIDE) for s in range(16)]


def limit(mib, **kw):
    return pltpu.CompilerParams(vmem_limit_bytes=mib * MIB, **kw)


SMEM = pl.BlockSpec(memory_space=pltpu.SMEM)
VMEM = pl.BlockSpec(memory_space=pltpu.VMEM)
ANY = pl.BlockSpec(memory_space=pl.ANY)


def normed(values, gain):
    scale = lax.rsqrt(jnp.mean(values * values, axis=-1, keepdims=True) + EPSILON)
    return values * scale * gain


def down_kernel(rows_ref, w_ref, gain_ref, rot_ref, a_ref, b_ref, q_ref):
    w = w_ref[...].reshape(2048, RANK)
    lat = jnp.dot(rows_ref[...], w, preferred_element_type=f32)
    lat = normed(lat, gain_ref[0]).astype(bf16)

    @pl.when(pl.program_id(0) == 0)
    def _():
        a_ref[0:128, :] = lat[0:128]
        a_ref[128:PIECE, :] = rot_ref[0]
        b_ref[0:128, :] = lat[128:256]
        b_ref[128:PIECE, :] = rot_ref[1]

    @pl.when(pl.program_id(0) == 1)
    def _():
        q_ref[...] = lat


def down(rows, w, gains, rot):
    piece = jax.ShapeDtypeStruct((PIECE, RANK), bf16)
    return pl.pallas_call(
        down_kernel,
        grid=(2,),
        in_specs=[
            pl.BlockSpec((ROWS, 2048), lambda n: (0, 0)),
            pl.BlockSpec((16, 1, 128, RANK), lambda n: (0, n, 0, 0)),
            pl.BlockSpec((1, 1, RANK), lambda n: (n, 0, 0)),
            pl.BlockSpec((2, 16, RANK), lambda n: (0, 0, 0)),
        ],
        out_specs=(
            pl.BlockSpec((PIECE, RANK), lambda n: (0, 0)),
            pl.BlockSpec((PIECE, RANK), lambda n: (0, 0)),
            pl.BlockSpec((ROWS, RANK), lambda n: (0, 0)),
        ),
        out_shape=(piece, piece, jax.ShapeDtypeStruct((ROWS, RANK), bf16)),
        compiler_params=limit(16, dimension_semantics=("arbitrary",)),
        name="down",
    )(rows, w, gains, rot)


def reader(low, high=None):
    def read(at, count):
        cut = low.shape[0]
        if at < cut:
            return low[at : at + count, :]
        return high[at - cut : at - cut + count, :]

    return read


def spot(yx_ref, i, j, half):
    at = ((yx_ref[0] - i + 4) % 4 * 4 + (yx_ref[1] - j + 4) % 4) * 256 + half * 128
    return pl.multiple_of(at, 128)


def expand(read, spots, w_ref, wvt_ref, k_ref, r_ref, vt_ref):
    rows = jnp.concatenate([read(PIECE * n, 128) for n in range(4)], axis=0)
    keys = jnp.dot(rows, w_ref[:, 0:512], preferred_element_type=f32).astype(bf16)
    values = lax.dot_general(
        wvt_ref[...], rows, (((1,), (1,)), ((), ())), preferred_element_type=f32
    ).astype(bf16)
    for n, at in enumerate(spots):
        for p in range(2):
            k_ref[p, pl.ds(at, 128), :] = keys[128 * n : 128 * n + 128, 256 * p : 256 * p + 256]
            vt_ref[p, :, pl.ds(at, 128)] = values[256 * p : 256 * p + 256, 128 * n : 128 * n + 128]
        packed = read(PIECE * n + 128, 16)
        rot = jnp.concatenate([packed[:, 64 * u : 64 * u + 64] for u in range(8)], axis=0)
        r_ref[pl.ds(at, 128), :] = jnp.concatenate([rot, jnp.zeros((128, 64), bf16)], axis=1)


def expand_queries(qn, i, w_ref, cos_ref, sin_ref, q_ref):
    both = jnp.dot(qn, w_ref[:, 1024:2048], preferred_element_type=f32)
    cosine = cos_ref[:, 128 * i : 128 * i + 128]
    sine = sin_ref[:, 128 * i : 128 * i + 128]
    cosine = jnp.concatenate([cosine, cosine], axis=1)
    sine = jnp.concatenate([sine, sine], axis=1)
    turned = (both[:, 512:768] * cosine + both[:, 768:1024] * sine).astype(bf16)
    pad = jnp.zeros((ROWS, 64), bf16)
    for h in range(LOCAL):
        q_ref[h, ROWS * i : ROWS * (i + 1), 0:128] = both[:, 128 * h : 128 * h + 128].astype(bf16)
        q_ref[h, ROWS * i : ROWS * (i + 1), 128:256] = jnp.concatenate(
            [turned[:, 64 * h : 64 * h + 64], pad], axis=1
        )


COL = 4 * PIECE
ROW = COL + ROWS
UP = 32


def early_kernel(
    yx_ref, a0, a1, a3, b0, b1, b3, own_w, other_w, cos_ref, sin_ref,
    k_ref, r_ref, vt_ref, q_ref, w_ref, wvt_ref, col_ref, row_ref, weight_ref, sems,
):
    copies = []
    for n, (source, target) in enumerate(
        [(own_w, weight_ref.at[0]), (other_w, weight_ref.at[1])]
        + [(piece, col_ref.at[n]) for n, piece in enumerate((a0, a1, a3))]
        + [(piece, row_ref.at[n]) for n, piece in enumerate((b0, b1, b3))]
    ):
        copies.append(pltpu.make_async_copy(source, target, sems.at[n]))
        copies[-1].start()
    z = yx_ref[2]
    core = yx_ref[3]
    copies[0].wait()
    copies[1].wait()
    for i in range(8):
        at = ((z - i + 8) % 8) * 2 * UP
        for k, part in ((0, core), (1, 1 - core)):
            spot_at = pl.multiple_of(at + part * UP, UP)
            w_ref[pl.ds(spot_at, UP), :] = weight_ref[k, UP * i : UP * (i + 1), :]
    wvt_ref[...] = w_ref[:, 512:1024].T
    outs = (w_ref, wvt_ref, k_ref, r_ref, vt_ref)
    for n, j in enumerate((0, 1, 3)):
        copies[2 + n].wait()
        expand(reader(col_ref.at[n]), [spot(yx_ref, i, j, 0) for i in range(4)], *outs)
    for n, i in enumerate((0, 1, 3)):
        copies[5 + n].wait()
        expand(reader(row_ref.at[n]), [spot(yx_ref, i, j, 1) for j in range(4)], *outs)
        expand_queries(row_ref[n, COL:ROW, :], i, w_ref, cos_ref, sin_ref, q_ref)


EXPANDED = (
    (2, LENGTH, 256),
    (LENGTH, 128),
    (2, 256, LENGTH),
    (LOCAL, SIDE * ROWS, 256),
)


def expand_early(yx, parts, w_own, w_other, cosine, sine):
    out = EXPANDED + ((RANK, 2048), (512, RANK))
    return pl.pallas_call(
        early_kernel,
        out_shape=tuple(jax.ShapeDtypeStruct(s, bf16) for s in out),
        in_specs=[SMEM] + [ANY] * 8 + [VMEM] * 2,
        out_specs=(VMEM,) * 6,
        scratch_shapes=[
            pltpu.VMEM((3, COL, RANK), bf16),
            pltpu.VMEM((3, ROW, RANK), bf16),
            pltpu.VMEM((2, 8 * UP, 2048), bf16),
            pltpu.SemaphoreType.DMA((8,)),
        ],
        compiler_params=limit(28),
        name="early",
    )(yx, *parts, w_own, w_other, cosine, sine)


KEYS = 512
PAIR = 2


def attend_kernel(
    yx_ref, a2l, a2h, b2l, b2h, cos_ref, sin_ref, k_in, r_in, vt_in, q_in, w_ref, wvt_ref,
    o0, o1, o2, o3, k_ref, r_ref, vt_ref, q_ref, score_ref, top_ref, sum_ref, acc_ref,
):
    pair = pl.program_id(0)
    step = pl.program_id(1)

    @pl.when((pair == 0) & (step == 0))
    def _():
        for p in range(2):
            k_ref[p] = k_in[p]
            vt_ref[p] = vt_in[p]
        r_ref[...] = r_in[...]
        for h in range(LOCAL):
            q_ref[h] = q_in[h]
        outs = (w_ref, wvt_ref, k_ref, r_ref, vt_ref)
        expand(reader(a2l, a2h), [spot(yx_ref, i, 2, 0) for i in range(4)], *outs)
        last = reader(b2l, b2h)
        expand(last, [spot(yx_ref, 2, j, 1) for j in range(4)], *outs)
        expand_queries(last(4 * PIECE, ROWS), 2, w_ref, cos_ref, sin_ref, q_ref)

    s = (yx_ref[0] - step + 4) % 4 * 4 + yx_ref[1]
    mine = pl.multiple_of(step * ROWS, ROWS)

    def score(at, slot, ahead):
        rot = r_ref[pl.ds(at, KEYS), :]
        for h in range(PAIR):
            keys = jnp.concatenate([k_ref[pair, pl.ds(at, KEYS), 128 * h : 128 * h + 128], rot], axis=1)
            query = q_ref[PAIR * pair + h, pl.ds(mine, ROWS), :]
            st = lax.dot_general(keys, query, (((1,), (1,)), ((), ())), preferred_element_type=f32)
            if ahead is not None:
                key_pos = lax.broadcasted_iota(jnp.int32, st.shape, 0)
                query_pos = lax.broadcasted_iota(jnp.int32, st.shape, 1)
                st = jnp.where(key_pos <= query_pos + ahead, st, -jnp.inf)
            score_ref[slot, h] = st

    def add(at, slot):
        for h in range(PAIR):
            st = score_ref[slot, h]
            top = top_ref[h]
            new = jnp.maximum(top, jnp.max(st, axis=0, keepdims=True))
            expo = jnp.exp2(st * SCALE2 - new * SCALE2)
            fade = jnp.exp2((top - new) * SCALE2)
            top_ref[h] = new
            sum_ref[h] = sum_ref[h] * fade + jnp.sum(expo, axis=0, keepdims=True)
            acc_ref[h] = acc_ref[h] * fade + jnp.dot(
                vt_ref[pair, 128 * h : 128 * h + 128, pl.ds(at, KEYS)],
                expo.astype(bf16),
                preferred_element_type=f32,
            )

    top_ref[...] = jnp.full(top_ref.shape, -jnp.inf, f32)
    sum_ref[...] = jnp.zeros(sum_ref.shape, f32)
    acc_ref[...] = jnp.zeros(acc_ref.shape, f32)
    full = s // 2
    last = pl.multiple_of(full * KEYS, KEYS)

    def at(j):
        return pl.multiple_of(j * KEYS, KEYS)

    def before(j):
        return pl.multiple_of(jnp.where(j == 0, full, j - 1) * KEYS, KEYS)

    score(last, 0, s * ROWS - last)

    def body(t, carry):
        j = 2 * t
        score(at(j), 1, None)
        add(before(j), 0)
        score(at(j + 1), 0, None)
        add(at(j), 1)
        return carry

    lax.fori_loop(0, full // 2, body, 0)

    @pl.when(full % 2 == 1)
    def _():
        score(at(full - 1), 1, None)
        add(before(full - 1), 0)
        add(at(full - 1), 1)

    @pl.when(full % 2 == 0)
    def _():
        add(before(full), 0)

    for i, o_ref in enumerate((o0, o1, o2, o3)):

        @pl.when(step == i)
        def _():
            for h in range(PAIR):
                o_ref[h * 128 : (h + 1) * 128, :] = (acc_ref[h] / sum_ref[h]).astype(bf16)


def attend(yx, halves, cosine, sine, early):
    piece = jax.ShapeDtypeStruct((LOCAL * 128, ROWS), bf16)
    return pl.pallas_call(
        attend_kernel,
        grid=(LOCAL // PAIR, SIDE),
        in_specs=[SMEM] + [VMEM] * 12,
        out_specs=(pl.BlockSpec((PAIR * 128, ROWS), lambda h, i: (h, 0)),) * SIDE,
        out_shape=(piece,) * SIDE,
        scratch_shapes=[pltpu.VMEM(s, bf16) for s in EXPANDED]
        + [
            pltpu.VMEM((2, PAIR, KEYS, ROWS), f32),
            pltpu.VMEM((PAIR, 1, ROWS), f32),
            pltpu.VMEM((PAIR, 1, ROWS), f32),
            pltpu.VMEM((PAIR, 128, ROWS), f32),
        ],
        compiler_params=limit(32, dimension_semantics=("arbitrary", "arbitrary")),
        name="attend",
    )(yx, *halves, cosine, sine, *early)


WIDE = 512


def out_kernel(y_ref, p0, p1, p2, p3, w_ref, gain_ref, o_ref, rows_ref, proj_ref):
    n = pl.program_id(0)
    y = y_ref[0]

    @pl.when(n == 0)
    def _():
        for i, piece in enumerate((p0, p1, p2, p3)):
            g = pl.multiple_of(((y + i) % 4) * 512, 512)
            rows_ref[:, pl.ds(g, 512)] = piece[...].T

    proj_ref[:, pl.ds(pl.multiple_of(n * WIDE, WIDE), WIDE)] = jnp.dot(
        rows_ref[...], w_ref[...], preferred_element_type=f32
    )

    @pl.when(n == pl.num_programs(0) - 1)
    def _():
        o_ref[...] = normed(proj_ref[...], gain_ref[...]).astype(bf16)


def project(y, pieces, w_out, gain):
    return pl.pallas_call(
        out_kernel,
        grid=(2048 // WIDE,),
        in_specs=[SMEM]
        + [pl.BlockSpec((512, ROWS), lambda n: (0, 0))] * 4
        + [
            pl.BlockSpec((2048, WIDE), lambda n: (0, n)),
            pl.BlockSpec((1, 2048), lambda n: (0, 0)),
        ],
        out_specs=pl.BlockSpec((ROWS, 2048), lambda n: (0, 0)),
        out_shape=jax.ShapeDtypeStruct((ROWS, 2048), bf16),
        scratch_shapes=[pltpu.VMEM((ROWS, 2048), bf16), pltpu.VMEM((ROWS, 2048), f32)],
        compiler_params=limit(24, dimension_semantics=("arbitrary",)),
        name="project",
    )(y, *pieces, w_out, gain)


def up_columns(w_qup, w_kvup, y):
    rows = w_qup.shape[0]
    q = lax.dynamic_slice_in_dim(w_qup, y * LOCAL * 192, LOCAL * 192, 1).reshape(rows, LOCAL, 192)
    kv = lax.dynamic_slice_in_dim(w_kvup, y * LOCAL * 256, LOCAL * 256, 1).reshape(rows, LOCAL, 256)
    first = q[..., 128:160]
    second = q[..., 160:192]
    parts = [
        kv[..., :128],
        kv[..., 128:],
        q[..., :128],
        jnp.concatenate([first, second], axis=-1),
        jnp.concatenate([-second, first], axis=-1),
    ]
    return jnp.concatenate([p.reshape(rows, -1) for p in parts], axis=1)


def body(tokens, w_qdown, w_kvdown, w_rotary, q_gain, kv_gain, w_qup, w_kvup, w_out, out_gain):
    sp_place = lax.axis_index("sp")
    y = sp_place // SIDE
    x = sp_place % SIDE
    own = tokens[0]
    w_down = lax.all_gather(jnp.stack([w_kvdown, w_qdown]), "dp")

    lanes = jnp.arange(SIDE * 32)
    spots = ((y - lanes // 32 + SIDE) % SIDE) * SIDE + x
    positions = (spots[None, :] * ROWS + jnp.arange(ROWS)[:, None]).astype(f32)
    freqs = THETA ** (-(2 * (lanes % 32)).astype(f32) / ROPE)
    angles = positions * freqs[None, :]
    cosine = jnp.cos(angles).reshape(ROWS, SIDE, 1, 32)
    sine = jnp.sin(angles).reshape(ROWS, SIDE, 1, 32)
    cos_wide = jnp.broadcast_to(cosine, (ROWS, SIDE, 4, 32)).reshape(ROWS, SIDE * 128)
    sin_wide = jnp.broadcast_to(sine, (ROWS, SIDE, 4, 32)).reshape(ROWS, SIDE * 128)

    turned = jnp.dot(own, w_rotary, preferred_element_type=f32)
    first = turned[:, :32]
    second = turned[:, 32:]
    cos_own = cos_wide[:, :32]
    sin_own = sin_wide[:, :32]
    key_rot = jnp.concatenate(
        [first * cos_own - second * sin_own, second * cos_own + first * sin_own], axis=-1
    ).astype(bf16)
    packed = key_rot.reshape(2, 8, 16, 64).transpose(0, 2, 1, 3).reshape(2, 16, 512)

    w_own = z_blocks(up_columns(w_qup, w_kvup, y))
    w_other = lax.ppermute(w_own, "dp", PARTNER)
    dp_place = lax.axis_index("dp")
    yx = jnp.stack([y, x, dp_place // 2, dp_place % 2])
    w_down, w_own, w_other, cos_wide, sin_wide, packed, yx = lax.optimization_barrier(
        (w_down, w_own, w_other, cos_wide, sin_wide, packed, yx)
    )
    w_full = lax.all_gather(w_out, "dp", axis=1, tiled=True)

    gains = jnp.stack([kv_gain, q_gain]).reshape(2, 1, RANK)
    a, b, qn = down(own, w_down, gains, packed)

    a1 = lax.ppermute(a, "sp", y_shift(1))
    a3 = lax.ppermute(a, "sp", y_shift(-1))
    b1 = lax.ppermute(b, "sp", x_shift(1))
    b3 = lax.ppermute(b, "sp", x_shift(-1))
    a2 = lax.ppermute(a1, "sp", y_shift(1))
    b2 = lax.ppermute(b3, "sp", x_shift(-1))
    a1, a2, a3, b1, b2, b3, qn = lax.optimization_barrier((a1, a2, a3, b1, b2, b3, qn))
    col = jnp.concatenate([a, a1, a2, a3], axis=0)
    row = jnp.concatenate([b, b1, b2, b3, qn], axis=0)
    col1 = lax.ppermute(col, "sp", x_shift(1))
    col3 = lax.ppermute(col, "sp", x_shift(-1))
    row1 = lax.ppermute(row, "sp", y_shift(1))
    row3 = lax.ppermute(row, "sp", y_shift(-1))
    col2l = lax.ppermute(col1[:288], "sp", x_shift(1))
    col2h = lax.ppermute(col3[288:], "sp", x_shift(-1))
    row2l = lax.ppermute(row1[:416], "sp", y_shift(1))
    row2h = lax.ppermute(row3[416:], "sp", y_shift(-1))

    early = expand_early(
        yx, (col, col1, col3, row, row1, row3), w_own, w_other, cos_wide, sin_wide
    )
    attended = attend(yx, (col2l, col2h, row2l, row2h), cos_wide, sin_wide, early)
    pieces = [attended[0]] + [
        lax.ppermute(attended[i], "sp", y_shift(-i)) for i in range(1, SIDE)
    ]
    mixed = project(y.reshape(1), pieces, w_full, out_gain.reshape(1, 2048))
    return mixed[None]


def solution(mesh):
    in_specs = (
        P("dp", "sp", None),
        P("dp", None),
        P("dp", None),
        P(),
        P(),
        P(),
        P("dp", None),
        P("dp", None),
        P(None, "dp"),
        P(),
    )
    out_specs = P("dp", "sp", None)
    return jax.shard_map(body, mesh=mesh, in_specs=in_specs, out_specs=out_specs, check_vma=False)
```

```python
import jax
import jax.numpy as jnp
from jax import lax
from jax.experimental import pallas as pl
from jax.experimental.pallas import tpu as pltpu
from jax.sharding import PartitionSpec as P

HEADS = 16
NOPE = 128
ROPE = 64
VDIM = 128
RANK = 512
ROWS = 256
SIDE = 4
LENGTH = 4096
LOCAL = HEADS // SIDE
PIECE = 144

EPSILON = 1e-06
THETA = 10000.0
LOG2E = 1.4426950408889634
SCALE2 = (NOPE + ROPE) ** (-0.5) * LOG2E
MIB = 2**20


f32 = jnp.float32
bf16 = jnp.bfloat16


PARTNER = [(d, d ^ 1) for d in range(16)]


def z_shift(k):
    return [(d, (d + 2 * k) % 16) for d in range(16)]


def z_blocks(w):
    blocks = [w] + [None] * 7
    ahead = behind = w
    for i in range(1, 4):
        ahead = lax.ppermute(ahead, "dp", z_shift(1))
        behind = lax.ppermute(behind, "dp", z_shift(-1))
        blocks[i] = ahead
        blocks[8 - i] = behind
    blocks[4] = lax.ppermute(ahead, "dp", z_shift(1))
    return jnp.concatenate(blocks, axis=0)


def y_shift(k):
    return [(s, (s + SIDE * k) % 16) for s in range(16)]


def x_shift(k):
    return [(s, (s // SIDE) * SIDE + (s % SIDE + k) % SIDE) for s in range(16)]


def limit(mib, **kw):
    return pltpu.CompilerParams(vmem_limit_bytes=mib * MIB, **kw)


SMEM = pl.BlockSpec(memory_space=pltpu.SMEM)
VMEM = pl.BlockSpec(memory_space=pltpu.VMEM)
ANY = pl.BlockSpec(memory_space=pl.ANY)


def normed(values, gain):
    scale = lax.rsqrt(jnp.mean(values * values, axis=-1, keepdims=True) + EPSILON)
    return values * scale * gain


def down_kernel(rows_ref, w_ref, gain_ref, rot_ref, a_ref, b_ref, q_ref):
    w = w_ref[...].reshape(2048, RANK)
    lat = jnp.dot(rows_ref[...], w, preferred_element_type=f32)
    lat = normed(lat, gain_ref[0]).astype(bf16)

    @pl.when(pl.program_id(0) == 0)
    def _():
        a_ref[0:128, :] = lat[0:128]
        a_ref[128:PIECE, :] = rot_ref[0]
        b_ref[0:128, :] = lat[128:256]
        b_ref[128:PIECE, :] = rot_ref[1]

    @pl.when(pl.program_id(0) == 1)
    def _():
        q_ref[...] = lat


def down(rows, w, gains, rot):
    piece = jax.ShapeDtypeStruct((PIECE, RANK), bf16)
    return pl.pallas_call(
        down_kernel,
        grid=(2,),
        in_specs=[
            pl.BlockSpec((ROWS, 2048), lambda n: (0, 0)),
            pl.BlockSpec((16, 1, 128, RANK), lambda n: (0, n, 0, 0)),
            pl.BlockSpec((1, 1, RANK), lambda n: (n, 0, 0)),
            pl.BlockSpec((2, 16, RANK), lambda n: (0, 0, 0)),
        ],
        out_specs=(
            pl.BlockSpec((PIECE, RANK), lambda n: (0, 0)),
            pl.BlockSpec((PIECE, RANK), lambda n: (0, 0)),
            pl.BlockSpec((ROWS, RANK), lambda n: (0, 0)),
        ),
        out_shape=(piece, piece, jax.ShapeDtypeStruct((ROWS, RANK), bf16)),
        compiler_params=limit(60, dimension_semantics=("arbitrary",)),
        name="down",
    )(rows, w, gains, rot)


def reader(low, high=None):
    def read(at, count):
        cut = low.shape[0]
        if at < cut:
            return low[at : at + count, :]
        return high[at - cut : at - cut + count, :]

    return read


def spot(yx_ref, i, j, half):
    at = ((yx_ref[0] - i + 4) % 4 * 4 + (yx_ref[1] - j + 4) % 4) * 256 + half * 128
    return pl.multiple_of(at, 128)


def expand(read, spots, w_ref, wvt_ref, k_ref, r_ref, vt_ref):
    rows = jnp.concatenate([read(PIECE * n, 128) for n in range(4)], axis=0)
    keys = jnp.dot(rows, w_ref[:, 0:512], preferred_element_type=f32).astype(bf16)
    values = lax.dot_general(
        wvt_ref[...], rows, (((1,), (1,)), ((), ())), preferred_element_type=f32
    ).astype(bf16)
    for n, at in enumerate(spots):
        for p in range(2):
            k_ref[p, pl.ds(at, 128), :] = keys[128 * n : 128 * n + 128, 256 * p : 256 * p + 256]
            vt_ref[p, :, pl.ds(at, 128)] = values[256 * p : 256 * p + 256, 128 * n : 128 * n + 128]
        packed = read(PIECE * n + 128, 16)
        rot = jnp.concatenate([packed[:, 64 * u : 64 * u + 64] for u in range(8)], axis=0)
        r_ref[pl.ds(at, 128), :] = jnp.concatenate([rot, jnp.zeros((128, 64), bf16)], axis=1)


def expand_queries(qn, i, w_ref, cos_ref, sin_ref, q_ref):
    both = jnp.dot(qn, w_ref[:, 1024:2048], preferred_element_type=f32)
    cosine = jnp.concatenate([cos_ref[:, 32 * i : 32 * i + 32]] * 8, axis=1)
    sine = jnp.concatenate([sin_ref[:, 32 * i : 32 * i + 32]] * 8, axis=1)
    turned = (both[:, 512:768] * cosine + both[:, 768:1024] * sine).astype(bf16)
    pad = jnp.zeros((ROWS, 64), bf16)
    for h in range(LOCAL):
        q_ref[h, ROWS * i : ROWS * (i + 1), 0:128] = both[:, 128 * h : 128 * h + 128].astype(bf16)
        q_ref[h, ROWS * i : ROWS * (i + 1), 128:256] = jnp.concatenate(
            [turned[:, 64 * h : 64 * h + 64], pad], axis=1
        )


COL = 4 * PIECE
ROW = COL + ROWS
UP = 32


def early_kernel(
    yx_ref, a0, a1, a3, b0, b1, b3, own_w, other_w, cos_ref, sin_ref,
    k_ref, r_ref, vt_ref, q_ref, w_ref, wvt_ref, col_ref, row_ref, weight_ref, sems,
):
    copies = []
    for n, (source, target) in enumerate(
        [(own_w, weight_ref.at[0]), (other_w, weight_ref.at[1])]
        + [(piece, col_ref.at[n]) for n, piece in enumerate((a0, a1, a3))]
        + [(piece, row_ref.at[n]) for n, piece in enumerate((b0, b1, b3))]
    ):
        copies.append(pltpu.make_async_copy(source, target, sems.at[n]))
        copies[-1].start()
    z = yx_ref[2]
    core = yx_ref[3]
    copies[0].wait()
    copies[1].wait()
    for i in range(8):
        at = ((z - i + 8) % 8) * 2 * UP
        for k, part in ((0, core), (1, 1 - core)):
            spot_at = pl.multiple_of(at + part * UP, UP)
            w_ref[pl.ds(spot_at, UP), :] = weight_ref[k, UP * i : UP * (i + 1), :]
    wvt_ref[...] = w_ref[:, 512:1024].T
    outs = (w_ref, wvt_ref, k_ref, r_ref, vt_ref)
    for n, j in enumerate((0, 1, 3)):
        copies[2 + n].wait()
        expand(reader(col_ref.at[n]), [spot(yx_ref, i, j, 0) for i in range(4)], *outs)
    for n, i in enumerate((0, 1, 3)):
        copies[5 + n].wait()
        expand(reader(row_ref.at[n]), [spot(yx_ref, i, j, 1) for j in range(4)], *outs)
        expand_queries(row_ref[n, COL:ROW, :], i, w_ref, cos_ref, sin_ref, q_ref)


EXPANDED = (
    (2, LENGTH, 256),
    (LENGTH, 128),
    (2, 256, LENGTH),
    (LOCAL, SIDE * ROWS, 256),
)


def expand_early(yx, parts, w_own, w_other, cosine, sine):
    out = EXPANDED + ((RANK, 2048), (512, RANK))
    return pl.pallas_call(
        early_kernel,
        out_shape=tuple(jax.ShapeDtypeStruct(s, bf16) for s in out),
        in_specs=[SMEM] + [ANY] * 8 + [VMEM] * 2,
        out_specs=(VMEM,) * 6,
        scratch_shapes=[
            pltpu.VMEM((3, COL, RANK), bf16),
            pltpu.VMEM((3, ROW, RANK), bf16),
            pltpu.VMEM((2, 8 * UP, 2048), bf16),
            pltpu.SemaphoreType.DMA((8,)),
        ],
        compiler_params=limit(28),
        name="early",
    )(yx, *parts, w_own, w_other, cosine, sine)


KEYS = 512
PAIR = 2


def attend_kernel(
    yx_ref, a2l, a2h, b2l, b2h, cos_ref, sin_ref, k_in, r_in, vt_in, q_in, w_ref, wvt_ref,
    o0, o1, o2, o3, k_ref, r_ref, vt_ref, q_ref, score_ref, top_ref, sum_ref, acc_ref,
):
    pair = pl.program_id(0)
    step = pl.program_id(1)

    @pl.when((pair == 0) & (step == 0))
    def _():
        for p in range(2):
            k_ref[p] = k_in[p]
            vt_ref[p] = vt_in[p]
        r_ref[...] = r_in[...]
        for h in range(LOCAL):
            q_ref[h] = q_in[h]
        outs = (w_ref, wvt_ref, k_ref, r_ref, vt_ref)
        expand(reader(a2l, a2h), [spot(yx_ref, i, 2, 0) for i in range(4)], *outs)
        last = reader(b2l, b2h)
        expand(last, [spot(yx_ref, 2, j, 1) for j in range(4)], *outs)
        expand_queries(last(4 * PIECE, ROWS), 2, w_ref, cos_ref, sin_ref, q_ref)

    s = (yx_ref[0] - step + 4) % 4 * 4 + yx_ref[1]
    mine = pl.multiple_of(step * ROWS, ROWS)

    def score(at, slot, ahead):
        rot = r_ref[pl.ds(at, KEYS), :]
        for h in range(PAIR):
            keys = jnp.concatenate([k_ref[pair, pl.ds(at, KEYS), 128 * h : 128 * h + 128], rot], axis=1)
            query = q_ref[PAIR * pair + h, pl.ds(mine, ROWS), :]
            st = lax.dot_general(keys, query, (((1,), (1,)), ((), ())), preferred_element_type=f32)
            if ahead is not None:
                key_pos = lax.broadcasted_iota(jnp.int32, st.shape, 0)
                query_pos = lax.broadcasted_iota(jnp.int32, st.shape, 1)
                st = jnp.where(key_pos <= query_pos + ahead, st, -jnp.inf)
            score_ref[slot, h] = st

    def add(at, slot):
        for h in range(PAIR):
            st = score_ref[slot, h]
            top = top_ref[h]
            new = jnp.maximum(top, jnp.max(st, axis=0, keepdims=True))
            expo = jnp.exp2(st * SCALE2 - new * SCALE2)
            fade = jnp.exp2((top - new) * SCALE2)
            top_ref[h] = new
            sum_ref[h] = sum_ref[h] * fade + jnp.sum(expo, axis=0, keepdims=True)
            acc_ref[h] = acc_ref[h] * fade + jnp.dot(
                vt_ref[pair, 128 * h : 128 * h + 128, pl.ds(at, KEYS)],
                expo.astype(bf16),
                preferred_element_type=f32,
            )

    top_ref[...] = jnp.full(top_ref.shape, -jnp.inf, f32)
    sum_ref[...] = jnp.zeros(sum_ref.shape, f32)
    acc_ref[...] = jnp.zeros(acc_ref.shape, f32)
    full = s // 2
    last = pl.multiple_of(full * KEYS, KEYS)

    def at(j):
        return pl.multiple_of(j * KEYS, KEYS)

    def before(j):
        return pl.multiple_of(jnp.where(j == 0, full, j - 1) * KEYS, KEYS)

    score(last, 0, s * ROWS - last)

    def body(t, carry):
        j = 2 * t
        score(at(j), 1, None)
        add(before(j), 0)
        score(at(j + 1), 0, None)
        add(at(j), 1)
        return carry

    lax.fori_loop(0, full // 2, body, 0)

    @pl.when(full % 2 == 1)
    def _():
        score(at(full - 1), 1, None)
        add(before(full - 1), 0)
        add(at(full - 1), 1)

    @pl.when(full % 2 == 0)
    def _():
        add(before(full), 0)

    for i, o_ref in enumerate((o0, o1, o2, o3)):

        @pl.when(step == i)
        def _():
            for h in range(PAIR):
                o_ref[h * 128 : (h + 1) * 128, :] = (acc_ref[h] / sum_ref[h]).astype(bf16)


def attend(yx, halves, cosine, sine, early):
    piece = jax.ShapeDtypeStruct((LOCAL * 128, ROWS), bf16)
    return pl.pallas_call(
        attend_kernel,
        grid=(LOCAL // PAIR, SIDE),
        in_specs=[SMEM] + [VMEM] * 12,
        out_specs=(pl.BlockSpec((PAIR * 128, ROWS), lambda h, i: (h, 0)),) * SIDE,
        out_shape=(piece,) * SIDE,
        scratch_shapes=[pltpu.VMEM(s, bf16) for s in EXPANDED]
        + [
            pltpu.VMEM((2, PAIR, KEYS, ROWS), f32),
            pltpu.VMEM((PAIR, 1, ROWS), f32),
            pltpu.VMEM((PAIR, 1, ROWS), f32),
            pltpu.VMEM((PAIR, 128, ROWS), f32),
        ],
        compiler_params=limit(32, dimension_semantics=("arbitrary", "arbitrary")),
        name="attend",
    )(yx, *halves, cosine, sine, *early)


WIDE = 512


def out_kernel(y_ref, p0, p1, p2, p3, w_ref, gain_ref, o_ref, rows_ref, proj_ref):
    n = pl.program_id(0)
    y = y_ref[0]

    @pl.when(n == 0)
    def _():
        for i, piece in enumerate((p0, p1, p2, p3)):
            g = pl.multiple_of(((y + i) % 4) * 512, 512)
            rows_ref[:, pl.ds(g, 512)] = piece[...].T

    proj_ref[:, pl.ds(pl.multiple_of(n * WIDE, WIDE), WIDE)] = jnp.dot(
        rows_ref[...], w_ref[...], preferred_element_type=f32
    )

    @pl.when(n == pl.num_programs(0) - 1)
    def _():
        o_ref[...] = normed(proj_ref[...], gain_ref[...]).astype(bf16)


def project(y, pieces, w_out, gain):
    return pl.pallas_call(
        out_kernel,
        grid=(2048 // WIDE,),
        in_specs=[SMEM]
        + [pl.BlockSpec((512, ROWS), lambda n: (0, 0))] * 4
        + [
            pl.BlockSpec((2048, WIDE), lambda n: (0, n)),
            pl.BlockSpec((1, 2048), lambda n: (0, 0)),
        ],
        out_specs=pl.BlockSpec((ROWS, 2048), lambda n: (0, 0)),
        out_shape=jax.ShapeDtypeStruct((ROWS, 2048), bf16),
        scratch_shapes=[pltpu.VMEM((ROWS, 2048), bf16), pltpu.VMEM((ROWS, 2048), f32)],
        compiler_params=limit(24, dimension_semantics=("arbitrary",)),
        name="project",
    )(y, *pieces, w_out, gain)


def stage_kernel(w_ref, o_ref, sem):
    copy = pltpu.make_async_copy(w_ref, o_ref, sem)
    copy.start()
    copy.wait()


def stage(w):
    return pl.pallas_call(
        stage_kernel,
        in_specs=[ANY],
        out_specs=VMEM,
        out_shape=jax.ShapeDtypeStruct(w.shape, w.dtype),
        scratch_shapes=[pltpu.SemaphoreType.DMA],
        compiler_params=limit(16),
        name="stage",
    )(w)


def up_columns(w_qup, w_kvup, y):
    rows = w_qup.shape[0]
    q = lax.dynamic_slice_in_dim(w_qup, y * LOCAL * 192, LOCAL * 192, 1).reshape(rows, LOCAL, 192)
    kv = lax.dynamic_slice_in_dim(w_kvup, y * LOCAL * 256, LOCAL * 256, 1).reshape(rows, LOCAL, 256)
    first = q[..., 128:160]
    second = q[..., 160:192]
    parts = [
        kv[..., :128],
        kv[..., 128:],
        q[..., :128],
        jnp.concatenate([first, second], axis=-1),
        jnp.concatenate([-second, first], axis=-1),
    ]
    return jnp.concatenate([p.reshape(rows, -1) for p in parts], axis=1)


def body(tokens, w_qdown, w_kvdown, w_rotary, q_gain, kv_gain, w_qup, w_kvup, w_out, out_gain):
    sp_place = lax.axis_index("sp")
    y = sp_place // SIDE
    x = sp_place % SIDE
    own = tokens[0]
    w_down = lax.all_gather(jnp.stack([w_kvdown, w_qdown]), "dp")

    lanes = jnp.arange(SIDE * 32)
    spots = ((y - lanes // 32 + SIDE) % SIDE) * SIDE + x
    positions = (spots[None, :] * ROWS + jnp.arange(ROWS)[:, None]).astype(f32)
    freqs = THETA ** (-(2 * (lanes % 32)).astype(f32) / ROPE)
    angles = positions * freqs[None, :]
    cosine = jnp.cos(angles)
    sine = jnp.sin(angles)

    turned = jnp.dot(own, w_rotary, preferred_element_type=f32)
    first = turned[:, :32]
    second = turned[:, 32:]
    cos_own = cosine[:, :32]
    sin_own = sine[:, :32]
    key_rot = jnp.concatenate(
        [first * cos_own - second * sin_own, second * cos_own + first * sin_own], axis=-1
    ).astype(bf16)
    packed = key_rot.reshape(2, 8, 16, 64).transpose(0, 2, 1, 3).reshape(2, 16, 512)

    w_own = z_blocks(up_columns(w_qup, w_kvup, y))
    w_other = lax.ppermute(w_own, "dp", PARTNER)
    dp_place = lax.axis_index("dp")
    yx = jnp.stack([y, x, dp_place // 2, dp_place % 2])
    w_down, w_own, w_other, cosine, sine, packed, yx = lax.optimization_barrier(
        (w_down, w_own, w_other, cosine, sine, packed, yx)
    )
    w_full = lax.all_gather(w_out, "dp", axis=1, tiled=True)

    gains = jnp.stack([kv_gain, q_gain]).reshape(2, 1, RANK)
    a, b, qn = down(own, w_down, gains, packed)

    a1 = lax.ppermute(a, "sp", y_shift(1))
    a3 = lax.ppermute(a, "sp", y_shift(-1))
    b1 = lax.ppermute(b, "sp", x_shift(1))
    b3 = lax.ppermute(b, "sp", x_shift(-1))
    a2 = lax.ppermute(a, "sp", y_shift(2))
    b2 = lax.ppermute(b, "sp", x_shift(2))
    a1, a2, a3, b1, b2, b3, qn = lax.optimization_barrier((a1, a2, a3, b1, b2, b3, qn))
    col = jnp.concatenate([a, a1, a2, a3], axis=0)
    row = jnp.concatenate([b, b1, b2, b3, qn], axis=0)
    col1 = lax.ppermute(col, "sp", x_shift(1))
    col3 = lax.ppermute(col, "sp", x_shift(-1))
    row1 = lax.ppermute(row, "sp", y_shift(1))
    row3 = lax.ppermute(row, "sp", y_shift(-1))
    col2l = lax.ppermute(col1[:288], "sp", x_shift(1))
    col2h = lax.ppermute(col3[288:], "sp", x_shift(-1))
    row2l = lax.ppermute(row1[:416], "sp", y_shift(1))
    row2h = lax.ppermute(row3[416:], "sp", y_shift(-1))

    early = expand_early(
        yx, (col, col1, col3, row, row1, row3), w_own, w_other, cosine, sine
    )
    attended = attend(yx, (col2l, col2h, row2l, row2h), cosine, sine, early)
    w_full, *attended = lax.optimization_barrier((w_full, *attended))
    pieces = [attended[0]] + [
        lax.ppermute(attended[i], "sp", y_shift(-i)) for i in range(1, SIDE)
    ]
    mixed = project(y.reshape(1), pieces, stage(w_full), out_gain.reshape(1, 2048))
    return mixed[None]


def solution(mesh):
    in_specs = (
        P("dp", "sp", None),
        P("dp", None),
        P("dp", None),
        P(),
        P(),
        P(),
        P("dp", None),
        P("dp", None),
        P(None, "dp"),
        P(),
    )
    out_specs = P("dp", "sp", None)
    return jax.shard_map(body, mesh=mesh, in_specs=in_specs, out_specs=out_specs, check_vma=False)
```

```python
import jax
import jax.numpy as jnp
from jax import lax
from jax.experimental import pallas as pl
from jax.experimental.pallas import tpu as pltpu
from jax.sharding import PartitionSpec as P


HEADS = 16
NOPE = 128
ROPE = 64
RANK = 512
ROWS = 256
SIDE = 4
LENGTH = 4096
LOCAL = HEADS // SIDE
PIECE = 144

EPSILON = 1e-06
THETA = 10000.0
LOG2E = 1.4426950408889634
SCALE2 = (NOPE + ROPE) ** (-0.5) * LOG2E
MIB = 2**20


f32 = jnp.float32
bf16 = jnp.bfloat16


PARTNER = [(d, d ^ 1) for d in range(16)]


def z_shift(k):
    return [(d, (d + 2 * k) % 16) for d in range(16)]


def z_blocks(w, first):
    blocks = [w] + [None] * 7
    ahead = behind = w
    for i in range(1, 4):
        ahead = lax.ppermute(ahead, "dp", z_shift(1))
        behind = lax.ppermute(behind, "dp", z_shift(-1))
        blocks[i] = ahead
        blocks[8 - i] = behind
    ahead, behind, *first = lax.optimization_barrier((ahead, behind, *first))
    blocks[4] = lax.ppermute(ahead, "dp", z_shift(1))
    return blocks, first


def y_shift(k):
    return [(s, (s + SIDE * k) % 16) for s in range(16)]


def x_shift(k):
    return [(s, (s // SIDE) * SIDE + (s % SIDE + k) % SIDE) for s in range(16)]


def limit(mib, **kw):
    return pltpu.CompilerParams(vmem_limit_bytes=mib * MIB, **kw)


SMEM = pl.BlockSpec(memory_space=pltpu.SMEM)
VMEM = pl.BlockSpec(memory_space=pltpu.VMEM)
ANY = pl.BlockSpec(memory_space=pl.ANY)


def normed(values, gain):
    scale = lax.rsqrt(jnp.mean(values * values, axis=-1, keepdims=True) + EPSILON)
    return values * scale * gain


def kv_down_kernel(rows_ref, w_ref, gain_ref, rot_ref, a_ref, b_ref, acc_ref):
    n = pl.program_id(0)
    part = jnp.dot(rows_ref[...], w_ref[...], preferred_element_type=f32)

    @pl.when(n == 0)
    def _():
        acc_ref[...] = part

    @pl.when(n > 0)
    def _():
        acc_ref[...] += part

    @pl.when(n == pl.num_programs(0) - 1)
    def _():
        lat = normed(acc_ref[...], gain_ref[...]).astype(bf16)
        a_ref[0:128, :] = lat[0:128]
        a_ref[128:PIECE, :] = rot_ref[0]
        b_ref[0:128, :] = lat[128:256]
        b_ref[128:PIECE, :] = rot_ref[1]


def kv_down(rows, w, gain, rot):
    piece = jax.ShapeDtypeStruct((PIECE, RANK), bf16)
    return pl.pallas_call(
        kv_down_kernel,
        grid=(2,),
        in_specs=[
            pl.BlockSpec((ROWS, 1024), lambda n: (0, n)),
            pl.BlockSpec((1024, RANK), lambda n: (n, 0)),
            pl.BlockSpec((1, RANK), lambda n: (0, 0)),
            pl.BlockSpec((2, 16, RANK), lambda n: (0, 0, 0)),
        ],
        out_specs=(pl.BlockSpec((PIECE, RANK), lambda n: (0, 0)),) * 2,
        out_shape=(piece, piece),
        scratch_shapes=[pltpu.VMEM((ROWS, RANK), f32)],
        compiler_params=limit(16, dimension_semantics=("arbitrary",)),
        name="kvdown",
    )(rows, w, gain, rot)


BLOCK = 256


def blocks_of(yx_ref, refs):
    z = yx_ref[2]
    core = yx_ref[3]
    for i in range(8):
        for ref, part in zip(refs, (core, 1 - core)):
            yield ref, BLOCK * i, ((z - i + 8) % 8) * 2 + part


def q_down_kernel(yx_ref, rows_ref, own_w, other_w, gain_ref, q_ref, w_ref):
    for ref, row, place in blocks_of(yx_ref, (own_w, other_w)):
        w_ref[pl.ds(pl.multiple_of(place * 128, 128), 128), :] = ref[row : row + 128, :]
    lat = jnp.dot(rows_ref[...], w_ref[...], preferred_element_type=f32)
    q_ref[...] = normed(lat, gain_ref[...]).astype(bf16)


def q_down(yx, rows, own_w, other_w, gain):
    return pl.pallas_call(
        q_down_kernel,
        in_specs=[SMEM] + [VMEM] * 4,
        out_specs=VMEM,
        out_shape=jax.ShapeDtypeStruct((ROWS, RANK), bf16),
        scratch_shapes=[pltpu.VMEM((2048, RANK), bf16)],
        compiler_params=limit(16),
        name="qdown",
    )(yx, rows, own_w, other_w, gain)


def reader(low, high=None):
    def read(at, count):
        cut = low.shape[0]
        if at < cut:
            return low[at : at + count, :]
        return high[at - cut : at - cut + count, :]

    return read


def spot(yx_ref, i, j, half):
    at = ((yx_ref[0] - i + 4) % 4 * 4 + (yx_ref[1] - j + 4) % 4) * 256 + half * 128
    return pl.multiple_of(at, 128)


def expand(read, spots, w_ref, wvt_ref, k_ref, r_ref, vt_ref):
    rows = jnp.concatenate([read(PIECE * n, 128) for n in range(4)], axis=0)
    keys = jnp.dot(rows, w_ref[:, 0:512], preferred_element_type=f32).astype(bf16)
    values = lax.dot_general(
        wvt_ref[...], rows, (((1,), (1,)), ((), ())), preferred_element_type=f32
    ).astype(bf16)
    for n, at in enumerate(spots):
        for p in range(2):
            k_ref[p, pl.ds(at, 128), :] = keys[128 * n : 128 * n + 128, 256 * p : 256 * p + 256]
            vt_ref[p, :, pl.ds(at, 128)] = values[256 * p : 256 * p + 256, 128 * n : 128 * n + 128]
        packed = read(PIECE * n + 128, 16)
        rot = jnp.concatenate([packed[:, 64 * u : 64 * u + 64] for u in range(8)], axis=0)
        r_ref[pl.ds(at, 128), :] = jnp.concatenate([rot, jnp.zeros((128, 64), bf16)], axis=1)


def expand_queries(qn, i, w_ref, cos_ref, sin_ref, q_ref):
    both = jnp.dot(qn, w_ref[:, 1024:2048], preferred_element_type=f32)
    cosine = jnp.concatenate([cos_ref[:, 32 * i : 32 * i + 32]] * 8, axis=1)
    sine = jnp.concatenate([sin_ref[:, 32 * i : 32 * i + 32]] * 8, axis=1)
    turned = (both[:, 512:768] * cosine + both[:, 768:1024] * sine).astype(bf16)
    pad = jnp.zeros((ROWS, 64), bf16)
    for h in range(LOCAL):
        q_ref[h, ROWS * i : ROWS * (i + 1), 0:128] = both[:, 128 * h : 128 * h + 128].astype(bf16)
        q_ref[h, ROWS * i : ROWS * (i + 1), 128:256] = jnp.concatenate(
            [turned[:, 64 * h : 64 * h + 64], pad], axis=1
        )


COL = 4 * PIECE
ROW = COL + ROWS
UP = 32


def early_kernel(
    yx_ref, a0, a1, a3, b0, b1, b3, own_w, other_w, cos_ref, sin_ref,
    k_ref, r_ref, vt_ref, q_ref, w_ref, wvt_ref, col_ref, row_ref, weight_ref, sems,
):
    copies = []
    for n, (source, target) in enumerate(
        [(own_w, weight_ref.at[0]), (other_w, weight_ref.at[1])]
        + [(piece, col_ref.at[n]) for n, piece in enumerate((a0, a1, a3))]
        + [(piece, row_ref.at[n]) for n, piece in enumerate((b0, b1, b3))]
    ):
        copies.append(pltpu.make_async_copy(source, target, sems.at[n]))
        copies[-1].start()
    copies[0].wait()
    copies[1].wait()
    for ref, row, place in blocks_of(yx_ref, (weight_ref.at[0], weight_ref.at[1])):
        at = pl.multiple_of(place * UP, UP)
        for g in range(4):
            rows = ref[row + 128 + UP * g : row + 128 + UP * (g + 1), :]
            w_ref[pl.ds(at, UP), 512 * g : 512 * (g + 1)] = rows
    wvt_ref[...] = w_ref[:, 512:1024].T
    outs = (w_ref, wvt_ref, k_ref, r_ref, vt_ref)
    for n, j in enumerate((0, 1, 3)):
        copies[2 + n].wait()
        expand(reader(col_ref.at[n]), [spot(yx_ref, i, j, 0) for i in range(4)], *outs)
    for n, i in enumerate((0, 1, 3)):
        copies[5 + n].wait()
        expand(reader(row_ref.at[n]), [spot(yx_ref, i, j, 1) for j in range(4)], *outs)
        expand_queries(row_ref[n, COL:ROW, :], i, w_ref, cos_ref, sin_ref, q_ref)


EXPANDED = (
    (2, LENGTH, 256),
    (LENGTH, 128),
    (2, 256, LENGTH),
    (LOCAL, SIDE * ROWS, 256),
)


def expand_early(yx, parts, w_own, w_other, cosine, sine):
    out = EXPANDED + ((RANK, 2048), (512, RANK))
    return pl.pallas_call(
        early_kernel,
        out_shape=tuple(jax.ShapeDtypeStruct(s, bf16) for s in out),
        in_specs=[SMEM] + [ANY] * 8 + [VMEM] * 2,
        out_specs=(VMEM,) * 6,
        scratch_shapes=[
            pltpu.VMEM((3, COL, RANK), bf16),
            pltpu.VMEM((3, ROW, RANK), bf16),
            pltpu.VMEM((2, 8 * BLOCK, RANK), bf16),
            pltpu.SemaphoreType.DMA((8,)),
        ],
        compiler_params=limit(28),
        name="early",
    )(yx, *parts, w_own, w_other, cosine, sine)


KEYS = 512
PAIR = 2


def attend_kernel(
    yx_ref, a2l, a2h, b2l, b2h, cos_ref, sin_ref, k_in, r_in, vt_in, q_in, w_ref, wvt_ref,
    o0, o1, o2, o3, k_ref, r_ref, vt_ref, q_ref, score_ref, top_ref, sum_ref, acc_ref,
):
    pair = pl.program_id(0)
    step = pl.program_id(1)

    @pl.when((pair == 0) & (step == 0))
    def _():
        for p in range(2):
            k_ref[p] = k_in[p]
            vt_ref[p] = vt_in[p]
        r_ref[...] = r_in[...]
        for h in range(LOCAL):
            q_ref[h] = q_in[h]
        outs = (w_ref, wvt_ref, k_ref, r_ref, vt_ref)
        expand(reader(a2l, a2h), [spot(yx_ref, i, 2, 0) for i in range(4)], *outs)
        last = reader(b2l, b2h)
        expand(last, [spot(yx_ref, 2, j, 1) for j in range(4)], *outs)
        expand_queries(last(4 * PIECE, ROWS), 2, w_ref, cos_ref, sin_ref, q_ref)

    s = (yx_ref[0] - step + 4) % 4 * 4 + yx_ref[1]
    mine = pl.multiple_of(step * ROWS, ROWS)

    def score(at, slot, ahead):
        rot = r_ref[pl.ds(at, KEYS), :]
        for h in range(PAIR):
            keys = jnp.concatenate([k_ref[pair, pl.ds(at, KEYS), 128 * h : 128 * h + 128], rot], axis=1)
            query = q_ref[PAIR * pair + h, pl.ds(mine, ROWS), :]
            st = lax.dot_general(keys, query, (((1,), (1,)), ((), ())), preferred_element_type=f32)
            if ahead is not None:
                key_pos = lax.broadcasted_iota(jnp.int32, st.shape, 0)
                query_pos = lax.broadcasted_iota(jnp.int32, st.shape, 1)
                st = jnp.where(key_pos <= query_pos + ahead, st, -jnp.inf)
            score_ref[slot, h] = st

    def add(at, slot):
        for h in range(PAIR):
            st = score_ref[slot, h]
            top = top_ref[h]
            new = jnp.maximum(top, jnp.max(st, axis=0, keepdims=True))
            expo = jnp.exp2(st * SCALE2 - new * SCALE2)
            fade = jnp.exp2((top - new) * SCALE2)
            top_ref[h] = new
            sum_ref[h] = sum_ref[h] * fade + jnp.sum(expo, axis=0, keepdims=True)
            acc_ref[h] = acc_ref[h] * fade + jnp.dot(
                vt_ref[pair, 128 * h : 128 * h + 128, pl.ds(at, KEYS)],
                expo.astype(bf16),
                preferred_element_type=f32,
            )

    top_ref[...] = jnp.full(top_ref.shape, -jnp.inf, f32)
    sum_ref[...] = jnp.zeros(sum_ref.shape, f32)
    acc_ref[...] = jnp.zeros(acc_ref.shape, f32)
    full = s // 2
    last = pl.multiple_of(full * KEYS, KEYS)

    def at(j):
        return pl.multiple_of(j * KEYS, KEYS)

    def before(j):
        return pl.multiple_of(jnp.where(j == 0, full, j - 1) * KEYS, KEYS)

    score(last, 0, s * ROWS - last)

    def body(t, carry):
        j = 2 * t
        score(at(j), 1, None)
        add(before(j), 0)
        score(at(j + 1), 0, None)
        add(at(j), 1)
        return carry

    lax.fori_loop(0, full // 2, body, 0)

    @pl.when(full % 2 == 1)
    def _():
        score(at(full - 1), 1, None)
        add(before(full - 1), 0)
        add(at(full - 1), 1)

    @pl.when(full % 2 == 0)
    def _():
        add(before(full), 0)

    for i, o_ref in enumerate((o0, o1, o2, o3)):

        @pl.when(step == i)
        def _():
            for h in range(PAIR):
                o_ref[h * 128 : (h + 1) * 128, :] = (acc_ref[h] / sum_ref[h]).astype(bf16)


def attend(yx, halves, cosine, sine, early):
    piece = jax.ShapeDtypeStruct((LOCAL * 128, ROWS), bf16)
    return pl.pallas_call(
        attend_kernel,
        grid=(LOCAL // PAIR, SIDE),
        in_specs=[SMEM] + [VMEM] * 12,
        out_specs=(pl.BlockSpec((PAIR * 128, ROWS), lambda h, i: (h, 0)),) * SIDE,
        out_shape=(piece,) * SIDE,
        scratch_shapes=[pltpu.VMEM(s, bf16) for s in EXPANDED]
        + [
            pltpu.VMEM((2, PAIR, KEYS, ROWS), f32),
            pltpu.VMEM((PAIR, 1, ROWS), f32),
            pltpu.VMEM((PAIR, 1, ROWS), f32),
            pltpu.VMEM((PAIR, 128, ROWS), f32),
        ],
        compiler_params=limit(32, dimension_semantics=("arbitrary", "arbitrary")),
        name="attend",
    )(yx, *halves, cosine, sine, *early)


WIDE = 512


def out_kernel(y_ref, p0, p1, p2, p3, w_ref, gain_ref, o_ref, rows_ref, proj_ref):
    n = pl.program_id(0)
    y = y_ref[0]

    @pl.when(n == 0)
    def _():
        for i, piece in enumerate((p0, p1, p2, p3)):
            g = pl.multiple_of(((y + i) % 4) * 512, 512)
            rows_ref[:, pl.ds(g, 512)] = piece[...].T

    proj_ref[:, pl.ds(pl.multiple_of(n * WIDE, WIDE), WIDE)] = jnp.dot(
        rows_ref[...], w_ref[...], preferred_element_type=f32
    )

    @pl.when(n == pl.num_programs(0) - 1)
    def _():
        o_ref[...] = normed(proj_ref[...], gain_ref[...]).astype(bf16)


def project(y, pieces, w_out, gain):
    return pl.pallas_call(
        out_kernel,
        grid=(2048 // WIDE,),
        in_specs=[SMEM]
        + [pl.BlockSpec((512, ROWS), lambda n: (0, 0))] * 4
        + [
            pl.BlockSpec((2048, WIDE), lambda n: (0, n)),
            pl.BlockSpec((1, 2048), lambda n: (0, 0)),
        ],
        out_specs=pl.BlockSpec((ROWS, 2048), lambda n: (0, 0)),
        out_shape=jax.ShapeDtypeStruct((ROWS, 2048), bf16),
        scratch_shapes=[pltpu.VMEM((ROWS, 2048), bf16), pltpu.VMEM((ROWS, 2048), f32)],
        compiler_params=limit(24, dimension_semantics=("arbitrary",)),
        name="project",
    )(y, *pieces, w_out, gain)


def stage_kernel(w_ref, o_ref, sem):
    copy = pltpu.make_async_copy(w_ref, o_ref, sem)
    copy.start()
    copy.wait()


def stage(w):
    return pl.pallas_call(
        stage_kernel,
        in_specs=[ANY],
        out_specs=VMEM,
        out_shape=jax.ShapeDtypeStruct(w.shape, w.dtype),
        scratch_shapes=[pltpu.SemaphoreType.DMA],
        compiler_params=limit(16),
        name="stage",
    )(w)


def up_columns(w_qup, w_kvup, y):
    rows = w_qup.shape[0]
    q = lax.dynamic_slice_in_dim(w_qup, y * LOCAL * 192, LOCAL * 192, 1).reshape(rows, LOCAL, 192)
    kv = lax.dynamic_slice_in_dim(w_kvup, y * LOCAL * 256, LOCAL * 256, 1).reshape(rows, LOCAL, 256)
    first = q[..., 128:160]
    second = q[..., 160:192]
    parts = [
        kv[..., :128],
        kv[..., 128:],
        q[..., :128],
        jnp.concatenate([first, second], axis=-1),
        jnp.concatenate([-second, first], axis=-1),
    ]
    queries = jnp.concatenate([p.reshape(rows, -1) for p in parts[3:]], axis=1)
    return [p.reshape(rows, 512) for p in parts[:3]] + [queries]


def body(tokens, w_qdown, w_kvdown, w_rotary, q_gain, kv_gain, w_qup, w_kvup, w_out, out_gain):
    sp_place = lax.axis_index("sp")
    y = sp_place // SIDE
    x = sp_place % SIDE
    own = tokens[0]
    w_kv = lax.all_gather(w_kvdown, "dp", axis=0, tiled=True)

    lanes = jnp.arange(SIDE * 32)
    spots = ((y - lanes // 32 + SIDE) % SIDE) * SIDE + x
    positions = (spots[None, :] * ROWS + jnp.arange(ROWS)[:, None]).astype(f32)
    freqs = THETA ** (-(2 * (lanes % 32)).astype(f32) / ROPE)
    angles = positions * freqs[None, :]
    cosine = jnp.cos(angles)
    sine = jnp.sin(angles)

    turned = jnp.dot(own, w_rotary, preferred_element_type=f32)
    first = turned[:, :32]
    second = turned[:, 32:]
    cos_own = cosine[:, :32]
    sin_own = sine[:, :32]
    key_rot = jnp.concatenate(
        [first * cos_own - second * sin_own, second * cos_own + first * sin_own], axis=-1
    ).astype(bf16)
    packed = key_rot.reshape(2, 8, 16, 64).transpose(0, 2, 1, 3).reshape(2, 16, 512)

    dp_place = lax.axis_index("dp")
    yx = jnp.stack([y, x, dp_place // 2, dp_place % 2])
    ring = jnp.concatenate([w_qdown] + up_columns(w_qup, w_kvup, y), axis=0)
    blocks, (w_kv, cosine, sine, packed, yx) = z_blocks(ring, (w_kv, cosine, sine, packed, yx))
    w_full = lax.all_gather(w_out, "dp", axis=1, tiled=True)

    a, b = kv_down(own, w_kv, kv_gain.reshape(1, RANK), packed)

    a1, a2, a3 = (lax.ppermute(a, "sp", y_shift(k)) for k in (1, 2, 3))
    b1, b2, b3 = (lax.ppermute(b, "sp", x_shift(k)) for k in (1, 2, 3))
    w_own = jnp.concatenate(blocks, axis=0)
    w_other = lax.ppermute(w_own, "dp", PARTNER)
    qn = q_down(yx, own, w_own, w_other, q_gain.reshape(1, RANK))
    a1, a2, a3, b1, b2, b3, qn = lax.optimization_barrier((a1, a2, a3, b1, b2, b3, qn))
    col = jnp.concatenate([a, a1, a2, a3], axis=0)
    row = jnp.concatenate([b, b1, b2, b3, qn], axis=0)
    col1 = lax.ppermute(col, "sp", x_shift(1))
    col3 = lax.ppermute(col, "sp", x_shift(-1))
    row1 = lax.ppermute(row, "sp", y_shift(1))
    row3 = lax.ppermute(row, "sp", y_shift(-1))
    col2l = lax.ppermute(col1[:288], "sp", x_shift(1))
    col2h = lax.ppermute(col3[288:], "sp", x_shift(-1))
    row2l = lax.ppermute(row1[:416], "sp", y_shift(1))
    row2h = lax.ppermute(row3[416:], "sp", y_shift(-1))

    early = expand_early(
        yx, (col, col1, col3, row, row1, row3), w_own, w_other, cosine, sine
    )
    attended = attend(yx, (col2l, col2h, row2l, row2h), cosine, sine, early)
    w_full, *attended = lax.optimization_barrier((w_full, *attended))
    pieces = [attended[0]] + [
        lax.ppermute(attended[i], "sp", y_shift(-i)) for i in range(1, SIDE)
    ]
    mixed = project(y.reshape(1), pieces, stage(w_full), out_gain.reshape(1, 2048))
    return mixed[None]


def solution(mesh):
    in_specs = (
        P("dp", "sp", None),
        P("dp", None),
        P("dp", None),
        P(),
        P(),
        P(),
        P("dp", None),
        P("dp", None),
        P(None, "dp"),
        P(),
    )
    out_specs = P("dp", "sp", None)

    return jax.shard_map(body, mesh=mesh, in_specs=in_specs, out_specs=out_specs, check_vma=False)
```

```python
import jax
import jax.numpy as jnp
from jax import lax
from jax.experimental import pallas as pl
from jax.experimental.pallas import tpu as pltpu
from jax.sharding import PartitionSpec as P

HEADS = 16
NOPE = 128
ROPE = 64
VDIM = 128
RANK = 512
ROWS = 256
SIDE = 4
LENGTH = 4096
LOCAL = HEADS // SIDE
PIECE = 144

EPSILON = 1e-06
THETA = 10000.0
LOG2E = 1.4426950408889634
SCALE2 = (NOPE + ROPE) ** (-0.5) * LOG2E
MIB = 2**20


f32 = jnp.float32
bf16 = jnp.bfloat16


PARTNER = [(d, d ^ 1) for d in range(16)]


def z_shift(k):
    return [(d, (d + 2 * k) % 16) for d in range(16)]


def z_blocks(w):
    blocks = [w] + [None] * 7
    ahead = behind = w
    for i in range(1, 4):
        ahead = lax.ppermute(ahead, "dp", z_shift(1))
        behind = lax.ppermute(behind, "dp", z_shift(-1))
        blocks[i] = ahead
        blocks[8 - i] = behind
    blocks[4] = lax.ppermute(ahead, "dp", z_shift(1))
    return jnp.concatenate(blocks, axis=0)


def y_shift(k):
    return [(s, (s + SIDE * k) % 16) for s in range(16)]


def x_shift(k):
    return [(s, (s // SIDE) * SIDE + (s % SIDE + k) % SIDE) for s in range(16)]


def limit(mib, **kw):
    return pltpu.CompilerParams(vmem_limit_bytes=mib * MIB, **kw)


SMEM = pl.BlockSpec(memory_space=pltpu.SMEM)
VMEM = pl.BlockSpec(memory_space=pltpu.VMEM)
ANY = pl.BlockSpec(memory_space=pl.ANY)


def normed(values, gain):
    scale = lax.rsqrt(jnp.mean(values * values, axis=-1, keepdims=True) + EPSILON)
    return values * scale * gain


def down_kernel(rows_ref, w_ref, gain_ref, rot_ref, a_ref, b_ref, q_ref):
    w = w_ref[...].reshape(2048, RANK)
    lat = jnp.dot(rows_ref[...], w, preferred_element_type=f32)
    lat = normed(lat, gain_ref[0]).astype(bf16)

    @pl.when(pl.program_id(0) == 0)
    def _():
        a_ref[0:128, :] = lat[0:128]
        a_ref[128:PIECE, :] = rot_ref[0]
        b_ref[0:128, :] = lat[128:256]
        b_ref[128:PIECE, :] = rot_ref[1]

    @pl.when(pl.program_id(0) == 1)
    def _():
        q_ref[...] = lat


def down(rows, w, gains, rot):
    piece = jax.ShapeDtypeStruct((PIECE, RANK), bf16)
    return pl.pallas_call(
        down_kernel,
        grid=(2,),
        in_specs=[
            pl.BlockSpec((ROWS, 2048), lambda n: (0, 0)),
            pl.BlockSpec((16, 1, 128, RANK), lambda n: (0, n, 0, 0)),
            pl.BlockSpec((1, 1, RANK), lambda n: (n, 0, 0)),
            pl.BlockSpec((2, 16, RANK), lambda n: (0, 0, 0)),
        ],
        out_specs=(
            pl.BlockSpec((PIECE, RANK), lambda n: (0, 0)),
            pl.BlockSpec((PIECE, RANK), lambda n: (0, 0)),
            pl.BlockSpec((ROWS, RANK), lambda n: (0, 0)),
        ),
        out_shape=(piece, piece, jax.ShapeDtypeStruct((ROWS, RANK), bf16)),
        compiler_params=limit(60, dimension_semantics=("arbitrary",)),
        name="down",
    )(rows, w, gains, rot)


def reader(low, high=None):
    def read(at, count):
        cut = low.shape[0]
        if at < cut:
            return low[at : at + count, :]
        return high[at - cut : at - cut + count, :]

    return read


def spot(yx_ref, i, j, half):
    at = ((yx_ref[0] - i + 4) % 4 * 4 + (yx_ref[1] - j + 4) % 4) * 256 + half * 128
    return pl.multiple_of(at, 128)


def expand(read, spots, w_ref, wvt_ref, k_ref, r_ref, vt_ref):
    rows = jnp.concatenate([read(PIECE * n, 128) for n in range(4)], axis=0)
    keys = jnp.dot(rows, w_ref[:, 0:512], preferred_element_type=f32).astype(bf16)
    values = lax.dot_general(
        wvt_ref[...], rows, (((1,), (1,)), ((), ())), preferred_element_type=f32
    ).astype(bf16)
    for n, at in enumerate(spots):
        for p in range(2):
            k_ref[p, pl.ds(at, 128), :] = keys[128 * n : 128 * n + 128, 256 * p : 256 * p + 256]
            vt_ref[p, :, pl.ds(at, 128)] = values[256 * p : 256 * p + 256, 128 * n : 128 * n + 128]
        packed = read(PIECE * n + 128, 16)
        rot = jnp.concatenate([packed[:, 64 * u : 64 * u + 64] for u in range(8)], axis=0)
        r_ref[pl.ds(at, 128), :] = jnp.concatenate([rot, jnp.zeros((128, 64), bf16)], axis=1)


def expand_queries(qn, i, w_ref, cos_ref, sin_ref, q_ref):
    both = jnp.dot(qn, w_ref[:, 1024:2048], preferred_element_type=f32)
    cosine = jnp.concatenate([cos_ref[:, 32 * i : 32 * i + 32]] * 8, axis=1)
    sine = jnp.concatenate([sin_ref[:, 32 * i : 32 * i + 32]] * 8, axis=1)
    turned = (both[:, 512:768] * cosine + both[:, 768:1024] * sine).astype(bf16)
    pad = jnp.zeros((ROWS, 64), bf16)
    for h in range(LOCAL):
        q_ref[h, ROWS * i : ROWS * (i + 1), 0:128] = both[:, 128 * h : 128 * h + 128].astype(bf16)
        q_ref[h, ROWS * i : ROWS * (i + 1), 128:256] = jnp.concatenate(
            [turned[:, 64 * h : 64 * h + 64], pad], axis=1
        )


COL = 4 * PIECE
ROW = COL + ROWS
UP = 32


def early_kernel(
    yx_ref, a0, a1, a3, b0, b1, b3, own_w, other_w, cos_ref, sin_ref,
    k_ref, r_ref, vt_ref, q_ref, w_ref, wvt_ref,
):
    z = yx_ref[2]
    core = yx_ref[3]
    for i in range(8):
        at = ((z - i + 8) % 8) * 2 * UP
        for ref, part in ((own_w, core), (other_w, 1 - core)):
            spot_at = pl.multiple_of(at + part * UP, UP)
            w_ref[pl.ds(spot_at, UP), :] = ref[UP * i : UP * (i + 1), :]
    wvt_ref[...] = w_ref[:, 512:1024].T
    outs = (w_ref, wvt_ref, k_ref, r_ref, vt_ref)
    for j, piece in ((0, a0), (1, a1), (3, a3)):
        expand(reader(piece), [spot(yx_ref, i, j, 0) for i in range(4)], *outs)
    for i, piece in ((0, b0), (1, b1), (3, b3)):
        expand(reader(piece), [spot(yx_ref, i, j, 1) for j in range(4)], *outs)
        expand_queries(piece[COL:ROW, :], i, w_ref, cos_ref, sin_ref, q_ref)


EXPANDED = (
    (2, LENGTH, 256),
    (LENGTH, 128),
    (2, 256, LENGTH),
    (LOCAL, SIDE * ROWS, 256),
)


def expand_early(yx, parts, w_own, w_other, cosine, sine):
    out = EXPANDED + ((RANK, 2048), (512, RANK))
    return pl.pallas_call(
        early_kernel,
        out_shape=tuple(jax.ShapeDtypeStruct(s, bf16) for s in out),
        in_specs=[SMEM] + [VMEM] * 10,
        out_specs=(VMEM,) * 6,
        compiler_params=limit(20),
        name="early",
    )(yx, *parts, w_own, w_other, cosine, sine)


KEYS = 512
PAIR = 2


def attend_kernel(
    yx_ref, a2l, a2h, b2l, b2h, cos_ref, sin_ref, k_in, r_in, vt_in, q_in, w_ref, wvt_ref,
    o0, o1, o2, o3, k_ref, r_ref, vt_ref, q_ref, score_ref, top_ref, sum_ref, acc_ref,
):
    pair = pl.program_id(0)
    step = pl.program_id(1)

    @pl.when((pair == 0) & (step == 0))
    def _():
        for p in range(2):
            k_ref[p] = k_in[p]
            vt_ref[p] = vt_in[p]
        r_ref[...] = r_in[...]
        for h in range(LOCAL):
            q_ref[h] = q_in[h]
        outs = (w_ref, wvt_ref, k_ref, r_ref, vt_ref)
        expand(reader(a2l, a2h), [spot(yx_ref, i, 2, 0) for i in range(4)], *outs)
        last = reader(b2l, b2h)
        expand(last, [spot(yx_ref, 2, j, 1) for j in range(4)], *outs)
        expand_queries(last(4 * PIECE, ROWS), 2, w_ref, cos_ref, sin_ref, q_ref)

    s = (yx_ref[0] - step + 4) % 4 * 4 + yx_ref[1]
    mine = pl.multiple_of(step * ROWS, ROWS)

    def score(at, slot, ahead):
        rot = r_ref[pl.ds(at, KEYS), :]
        for h in range(PAIR):
            keys = jnp.concatenate([k_ref[pair, pl.ds(at, KEYS), 128 * h : 128 * h + 128], rot], axis=1)
            query = q_ref[PAIR * pair + h, pl.ds(mine, ROWS), :]
            st = lax.dot_general(keys, query, (((1,), (1,)), ((), ())), preferred_element_type=f32)
            if ahead is not None:
                key_pos = lax.broadcasted_iota(jnp.int32, st.shape, 0)
                query_pos = lax.broadcasted_iota(jnp.int32, st.shape, 1)
                st = jnp.where(key_pos <= query_pos + ahead, st, -jnp.inf)
            score_ref[slot, h] = st

    def add(at, slot):
        for h in range(PAIR):
            st = score_ref[slot, h]
            top = top_ref[h]
            new = jnp.maximum(top, jnp.max(st, axis=0, keepdims=True))
            expo = jnp.exp2(st * SCALE2 - new * SCALE2)
            fade = jnp.exp2((top - new) * SCALE2)
            top_ref[h] = new
            sum_ref[h] = sum_ref[h] * fade + jnp.sum(expo, axis=0, keepdims=True)
            acc_ref[h] = acc_ref[h] * fade + jnp.dot(
                vt_ref[pair, 128 * h : 128 * h + 128, pl.ds(at, KEYS)],
                expo.astype(bf16),
                preferred_element_type=f32,
            )

    top_ref[...] = jnp.full(top_ref.shape, -jnp.inf, f32)
    sum_ref[...] = jnp.zeros(sum_ref.shape, f32)
    acc_ref[...] = jnp.zeros(acc_ref.shape, f32)
    full = s // 2
    last = pl.multiple_of(full * KEYS, KEYS)

    def at(j):
        return pl.multiple_of(j * KEYS, KEYS)

    def before(j):
        return pl.multiple_of(jnp.where(j == 0, full, j - 1) * KEYS, KEYS)

    score(last, 0, s * ROWS - last)

    def body(t, carry):
        j = 2 * t
        score(at(j), 1, None)
        add(before(j), 0)
        score(at(j + 1), 0, None)
        add(at(j), 1)
        return carry

    lax.fori_loop(0, full // 2, body, 0)

    @pl.when(full % 2 == 1)
    def _():
        score(at(full - 1), 1, None)
        add(before(full - 1), 0)
        add(at(full - 1), 1)

    @pl.when(full % 2 == 0)
    def _():
        add(before(full), 0)

    for i, o_ref in enumerate((o0, o1, o2, o3)):

        @pl.when(step == i)
        def _():
            for h in range(PAIR):
                o_ref[h * 128 : (h + 1) * 128, :] = (acc_ref[h] / sum_ref[h]).astype(bf16)


def attend(yx, halves, cosine, sine, early):
    piece = jax.ShapeDtypeStruct((LOCAL * 128, ROWS), bf16)
    return pl.pallas_call(
        attend_kernel,
        grid=(LOCAL // PAIR, SIDE),
        in_specs=[SMEM] + [VMEM] * 12,
        out_specs=(pl.BlockSpec((PAIR * 128, ROWS), lambda h, i: (h, 0)),) * SIDE,
        out_shape=(piece,) * SIDE,
        scratch_shapes=[pltpu.VMEM(s, bf16) for s in EXPANDED]
        + [
            pltpu.VMEM((2, PAIR, KEYS, ROWS), f32),
            pltpu.VMEM((PAIR, 1, ROWS), f32),
            pltpu.VMEM((PAIR, 1, ROWS), f32),
            pltpu.VMEM((PAIR, 128, ROWS), f32),
        ],
        compiler_params=limit(32, dimension_semantics=("arbitrary", "arbitrary")),
        name="attend",
    )(yx, *halves, cosine, sine, *early)


WIDE = 512


def out_kernel(y_ref, p0, p1, p2, p3, w_ref, gain_ref, o_ref, rows_ref, proj_ref):
    y = y_ref[0]
    for i, piece in enumerate((p0, p1, p2, p3)):
        g = pl.multiple_of(((y + i) % 4) * 512, 512)
        rows_ref[:, pl.ds(g, 512)] = piece[...].T
    for n in range(0, 2048, WIDE):
        proj_ref[:, n : n + WIDE] = jnp.dot(
            rows_ref[...], w_ref[:, n : n + WIDE], preferred_element_type=f32
        )
    o_ref[...] = normed(proj_ref[...], gain_ref[...]).astype(bf16)


def project(y, pieces, w_out, gain):
    return pl.pallas_call(
        out_kernel,
        in_specs=[SMEM] + [VMEM] * 6,
        out_specs=VMEM,
        out_shape=jax.ShapeDtypeStruct((ROWS, 2048), bf16),
        scratch_shapes=[pltpu.VMEM((ROWS, 2048), bf16), pltpu.VMEM((ROWS, 2048), f32)],
        compiler_params=limit(16),
        name="project",
    )(y, *pieces, w_out, gain)


def stage_kernel(w_ref, o_ref, sem):
    copy = pltpu.make_async_copy(w_ref, o_ref, sem)
    copy.start()
    copy.wait()


def stage(w):
    return pl.pallas_call(
        stage_kernel,
        in_specs=[ANY],
        out_specs=VMEM,
        out_shape=jax.ShapeDtypeStruct(w.shape, w.dtype),
        scratch_shapes=[pltpu.SemaphoreType.DMA],
        compiler_params=limit(16),
        name="stage",
    )(w)


def up_columns(w_qup, w_kvup, y):
    rows = w_qup.shape[0]
    q = lax.dynamic_slice_in_dim(w_qup, y * LOCAL * 192, LOCAL * 192, 1).reshape(rows, LOCAL, 192)
    kv = lax.dynamic_slice_in_dim(w_kvup, y * LOCAL * 256, LOCAL * 256, 1).reshape(rows, LOCAL, 256)
    first = q[..., 128:160]
    second = q[..., 160:192]
    parts = [
        kv[..., :128],
        kv[..., 128:],
        q[..., :128],
        jnp.concatenate([first, second], axis=-1),
        jnp.concatenate([-second, first], axis=-1),
    ]
    return jnp.concatenate([p.reshape(rows, -1) for p in parts], axis=1)


def body(tokens, w_qdown, w_kvdown, w_rotary, q_gain, kv_gain, w_qup, w_kvup, w_out, out_gain):
    sp_place = lax.axis_index("sp")
    y = sp_place // SIDE
    x = sp_place % SIDE
    own = tokens[0]
    w_down = lax.all_gather(jnp.stack([w_kvdown, w_qdown]), "dp")

    lanes = jnp.arange(SIDE * 32)
    spots = ((y - lanes // 32 + SIDE) % SIDE) * SIDE + x
    positions = (spots[None, :] * ROWS + jnp.arange(ROWS)[:, None]).astype(f32)
    freqs = THETA ** (-(2 * (lanes % 32)).astype(f32) / ROPE)
    angles = positions * freqs[None, :]
    cosine = jnp.cos(angles)
    sine = jnp.sin(angles)

    turned = jnp.dot(own, w_rotary, preferred_element_type=f32)
    first = turned[:, :32]
    second = turned[:, 32:]
    cos_own = cosine[:, :32]
    sin_own = sine[:, :32]
    key_rot = jnp.concatenate(
        [first * cos_own - second * sin_own, second * cos_own + first * sin_own], axis=-1
    ).astype(bf16)
    packed = key_rot.reshape(2, 8, 16, 64).transpose(0, 2, 1, 3).reshape(2, 16, 512)

    w_own = z_blocks(up_columns(w_qup, w_kvup, y))
    w_other = lax.ppermute(w_own, "dp", PARTNER)
    dp_place = lax.axis_index("dp")
    yx = jnp.stack([y, x, dp_place // 2, dp_place % 2])
    w_down, w_own, w_other, cosine, sine, packed, yx = lax.optimization_barrier(
        (w_down, w_own, w_other, cosine, sine, packed, yx)
    )
    w_full = lax.all_gather(w_out, "dp", axis=1, tiled=True)

    gains = jnp.stack([kv_gain, q_gain]).reshape(2, 1, RANK)
    a, b, qn = down(own, w_down, gains, packed)

    a1 = lax.ppermute(a, "sp", y_shift(1))
    a3 = lax.ppermute(a, "sp", y_shift(-1))
    b1 = lax.ppermute(b, "sp", x_shift(1))
    b3 = lax.ppermute(b, "sp", x_shift(-1))
    a2 = lax.ppermute(a, "sp", y_shift(2))
    b2 = lax.ppermute(b, "sp", x_shift(2))
    a1, a2, a3, b1, b2, b3, qn = lax.optimization_barrier((a1, a2, a3, b1, b2, b3, qn))
    col = jnp.concatenate([a, a1, a2, a3], axis=0)
    row = jnp.concatenate([b, b1, b2, b3, qn], axis=0)
    col1 = lax.ppermute(col, "sp", x_shift(1))
    col3 = lax.ppermute(col, "sp", x_shift(-1))
    row1 = lax.ppermute(row, "sp", y_shift(1))
    row3 = lax.ppermute(row, "sp", y_shift(-1))
    col2l = lax.ppermute(col1[:288], "sp", x_shift(1))
    col2h = lax.ppermute(col3[288:], "sp", x_shift(-1))
    row2l = lax.ppermute(row1[:416], "sp", y_shift(1))
    row2h = lax.ppermute(row3[416:], "sp", y_shift(-1))

    early = expand_early(
        yx, (col, col1, col3, row, row1, row3), w_own, w_other, cosine, sine
    )
    attended = attend(yx, (col2l, col2h, row2l, row2h), cosine, sine, early)
    w_full, *attended = lax.optimization_barrier((w_full, *attended))
    pieces = [attended[0]] + [
        lax.ppermute(attended[i], "sp", y_shift(-i)) for i in range(1, SIDE)
    ]
    mixed = project(y.reshape(1), pieces, stage(w_full), out_gain.reshape(1, 2048))
    return mixed[None]


def solution(mesh):
    in_specs = (
        P("dp", "sp", None),
        P("dp", None),
        P("dp", None),
        P(),
        P(),
        P(),
        P("dp", None),
        P("dp", None),
        P(None, "dp"),
        P(),
    )
    out_specs = P("dp", "sp", None)
    return jax.shard_map(body, mesh=mesh, in_specs=in_specs, out_specs=out_specs, check_vma=False)
```

```python
import jax
import jax.numpy as jnp
from jax import lax
from jax.experimental import pallas as pl
from jax.experimental.pallas import tpu as pltpu
from jax.sharding import PartitionSpec as P


HEADS = 16
NOPE = 128
ROPE = 64
RANK = 512
ROWS = 256
SIDE = 4
LENGTH = 4096
LOCAL = HEADS // SIDE
PIECE = 144

EPSILON = 1e-06
THETA = 10000.0
LOG2E = 1.4426950408889634
SCALE2 = (NOPE + ROPE) ** (-0.5) * LOG2E
MIB = 2**20


f32 = jnp.float32
bf16 = jnp.bfloat16


PARTNER = [(d, d ^ 1) for d in range(16)]


def z_shift(k):
    return [(d, (d + 2 * k) % 16) for d in range(16)]


def z_blocks(w):
    blocks = [w] + [None] * 7
    ahead = behind = w
    for i in range(1, 4):
        ahead = lax.ppermute(ahead, "dp", z_shift(1))
        behind = lax.ppermute(behind, "dp", z_shift(-1))
        blocks[i] = ahead
        blocks[8 - i] = behind
    blocks[4] = lax.ppermute(ahead, "dp", z_shift(1))
    return jnp.concatenate(blocks, axis=0)


def y_shift(k):
    return [(s, (s + SIDE * k) % 16) for s in range(16)]


def x_shift(k):
    return [(s, (s // SIDE) * SIDE + (s % SIDE + k) % SIDE) for s in range(16)]


def limit(mib, **kw):
    return pltpu.CompilerParams(vmem_limit_bytes=mib * MIB, **kw)


SMEM = pl.BlockSpec(memory_space=pltpu.SMEM)
VMEM = pl.BlockSpec(memory_space=pltpu.VMEM)
ANY = pl.BlockSpec(memory_space=pl.ANY)


def normed(values, gain):
    scale = lax.rsqrt(jnp.mean(values * values, axis=-1, keepdims=True) + EPSILON)
    return values * scale * gain


def down_kernel(rows_ref, w_ref, gain_ref, rot_ref, a_ref, b_ref, q_ref, acc_ref):
    n = pl.program_id(0)
    k = pl.program_id(1)
    w = w_ref[...].reshape(512, RANK)
    part = jnp.dot(rows_ref[...], w, preferred_element_type=f32)

    @pl.when(k == 0)
    def _():
        acc_ref[...] = part

    @pl.when(k > 0)
    def _():
        acc_ref[...] += part

    @pl.when(k == pl.num_programs(1) - 1)
    def _():
        lat = normed(acc_ref[...], gain_ref[0]).astype(bf16)

        @pl.when(n == 0)
        def _():
            a_ref[0:128, :] = lat[0:128]
            a_ref[128:PIECE, :] = rot_ref[0]
            b_ref[0:128, :] = lat[128:256]
            b_ref[128:PIECE, :] = rot_ref[1]

        @pl.when(n == 1)
        def _():
            q_ref[...] = lat


def down(rows, w, gains, rot):
    piece = jax.ShapeDtypeStruct((PIECE, RANK), bf16)
    return pl.pallas_call(
        down_kernel,
        grid=(2, 4),
        in_specs=[
            pl.BlockSpec((ROWS, 512), lambda n, k: (0, k)),
            pl.BlockSpec((4, 1, 128, RANK), lambda n, k: (k, n, 0, 0)),
            pl.BlockSpec((1, 1, RANK), lambda n, k: (n, 0, 0)),
            pl.BlockSpec((2, 16, RANK), lambda n, k: (0, 0, 0)),
        ],
        out_specs=(
            pl.BlockSpec((PIECE, RANK), lambda n, k: (0, 0)),
            pl.BlockSpec((PIECE, RANK), lambda n, k: (0, 0)),
            pl.BlockSpec((ROWS, RANK), lambda n, k: (0, 0)),
        ),
        out_shape=(piece, piece, jax.ShapeDtypeStruct((ROWS, RANK), bf16)),
        scratch_shapes=[pltpu.VMEM((ROWS, RANK), f32)],
        compiler_params=limit(60, dimension_semantics=("arbitrary", "arbitrary")),
        name="down",
    )(rows, w, gains, rot)


def reader(low, high=None):
    def read(at, count):
        cut = low.shape[0]
        if at < cut:
            return low[at : at + count, :]
        return high[at - cut : at - cut + count, :]

    return read


def spot(yx_ref, i, j, half):
    at = ((yx_ref[0] - i + 4) % 4 * 4 + (yx_ref[1] - j + 4) % 4) * 256 + half * 128
    return pl.multiple_of(at, 128)


def expand(read, spots, w_ref, wvt_ref, k_ref, r_ref, vt_ref):
    rows = jnp.concatenate([read(PIECE * n, 128) for n in range(4)], axis=0)
    keys = jnp.dot(rows, w_ref[:, 0:512], preferred_element_type=f32).astype(bf16)
    values = lax.dot_general(
        wvt_ref[...], rows, (((1,), (1,)), ((), ())), preferred_element_type=f32
    ).astype(bf16)
    for n, at in enumerate(spots):
        for p in range(2):
            k_ref[p, pl.ds(at, 128), :] = keys[128 * n : 128 * n + 128, 256 * p : 256 * p + 256]
            vt_ref[p, :, pl.ds(at, 128)] = values[256 * p : 256 * p + 256, 128 * n : 128 * n + 128]
        packed = read(PIECE * n + 128, 16)
        rot = jnp.concatenate([packed[:, 64 * u : 64 * u + 64] for u in range(8)], axis=0)
        r_ref[pl.ds(at, 128), :] = jnp.concatenate([rot, jnp.zeros((128, 64), bf16)], axis=1)


def expand_queries(qn, i, w_ref, cos_ref, sin_ref, q_ref):
    both = jnp.dot(qn, w_ref[:, 1024:2048], preferred_element_type=f32)
    cosine = jnp.concatenate([cos_ref[:, 32 * i : 32 * i + 32]] * 8, axis=1)
    sine = jnp.concatenate([sin_ref[:, 32 * i : 32 * i + 32]] * 8, axis=1)
    turned = (both[:, 512:768] * cosine + both[:, 768:1024] * sine).astype(bf16)
    pad = jnp.zeros((ROWS, 64), bf16)
    for h in range(LOCAL):
        q_ref[h, ROWS * i : ROWS * (i + 1), 0:128] = both[:, 128 * h : 128 * h + 128].astype(bf16)
        q_ref[h, ROWS * i : ROWS * (i + 1), 128:256] = jnp.concatenate(
            [turned[:, 64 * h : 64 * h + 64], pad], axis=1
        )


COL = 4 * PIECE
ROW = COL + ROWS
UP = 32


def early_kernel(
    yx_ref, a0, a1, a3, b0, b1, b3, own_w, other_w, cos_ref, sin_ref,
    k_ref, r_ref, vt_ref, q_ref, w_ref, wvt_ref,
):
    z = yx_ref[2]
    core = yx_ref[3]
    for i in range(8):
        at = ((z - i + 8) % 8) * 2 * UP
        for ref, part in ((own_w, core), (other_w, 1 - core)):
            spot_at = pl.multiple_of(at + part * UP, UP)
            w_ref[pl.ds(spot_at, UP), :] = ref[UP * i : UP * (i + 1), :]
    wvt_ref[...] = w_ref[:, 512:1024].T
    outs = (w_ref, wvt_ref, k_ref, r_ref, vt_ref)
    for j, piece in ((0, a0), (1, a1), (3, a3)):
        expand(reader(piece), [spot(yx_ref, i, j, 0) for i in range(4)], *outs)
    for i, piece in ((0, b0), (1, b1), (3, b3)):
        expand(reader(piece), [spot(yx_ref, i, j, 1) for j in range(4)], *outs)
        expand_queries(piece[COL:ROW, :], i, w_ref, cos_ref, sin_ref, q_ref)


EXPANDED = (
    (2, LENGTH, 256),
    (LENGTH, 128),
    (2, 256, LENGTH),
    (LOCAL, SIDE * ROWS, 256),
)


def expand_early(yx, parts, w_own, w_other, cosine, sine):
    out = EXPANDED + ((RANK, 2048), (512, RANK))
    return pl.pallas_call(
        early_kernel,
        out_shape=tuple(jax.ShapeDtypeStruct(s, bf16) for s in out),
        in_specs=[SMEM] + [VMEM] * 10,
        out_specs=(VMEM,) * 6,
        compiler_params=limit(20),
        name="early",
    )(yx, *parts, w_own, w_other, cosine, sine)


KEYS = 512
PAIR = 2


def attend_kernel(
    yx_ref, a2l, a2h, b2l, b2h, cos_ref, sin_ref, k_in, r_in, vt_in, q_in, w_ref, wvt_ref,
    o0, o1, o2, o3, k_ref, r_ref, vt_ref, q_ref, score_ref, top_ref, sum_ref, acc_ref,
):
    pair = pl.program_id(0)
    step = pl.program_id(1)

    @pl.when((pair == 0) & (step == 0))
    def _():
        for p in range(2):
            k_ref[p] = k_in[p]
            vt_ref[p] = vt_in[p]
        r_ref[...] = r_in[...]
        for h in range(LOCAL):
            q_ref[h] = q_in[h]
        outs = (w_ref, wvt_ref, k_ref, r_ref, vt_ref)
        expand(reader(a2l, a2h), [spot(yx_ref, i, 2, 0) for i in range(4)], *outs)
        last = reader(b2l, b2h)
        expand(last, [spot(yx_ref, 2, j, 1) for j in range(4)], *outs)
        expand_queries(last(4 * PIECE, ROWS), 2, w_ref, cos_ref, sin_ref, q_ref)

    s = (yx_ref[0] - step + 4) % 4 * 4 + yx_ref[1]
    mine = pl.multiple_of(step * ROWS, ROWS)

    def score(at, slot, ahead):
        rot = r_ref[pl.ds(at, KEYS), :]
        for h in range(PAIR):
            keys = jnp.concatenate([k_ref[pair, pl.ds(at, KEYS), 128 * h : 128 * h + 128], rot], axis=1)
            query = q_ref[PAIR * pair + h, pl.ds(mine, ROWS), :]
            st = lax.dot_general(keys, query, (((1,), (1,)), ((), ())), preferred_element_type=f32)
            if ahead is not None:
                key_pos = lax.broadcasted_iota(jnp.int32, st.shape, 0)
                query_pos = lax.broadcasted_iota(jnp.int32, st.shape, 1)
                st = jnp.where(key_pos <= query_pos + ahead, st, -jnp.inf)
            score_ref[slot, h] = st

    def add(at, slot):
        for h in range(PAIR):
            st = score_ref[slot, h]
            top = top_ref[h]
            new = jnp.maximum(top, jnp.max(st, axis=0, keepdims=True))
            expo = jnp.exp2(st * SCALE2 - new * SCALE2)
            fade = jnp.exp2((top - new) * SCALE2)
            top_ref[h] = new
            sum_ref[h] = sum_ref[h] * fade + jnp.sum(expo, axis=0, keepdims=True)
            acc_ref[h] = acc_ref[h] * fade + jnp.dot(
                vt_ref[pair, 128 * h : 128 * h + 128, pl.ds(at, KEYS)],
                expo.astype(bf16),
                preferred_element_type=f32,
            )

    top_ref[...] = jnp.full(top_ref.shape, -jnp.inf, f32)
    sum_ref[...] = jnp.zeros(sum_ref.shape, f32)
    acc_ref[...] = jnp.zeros(acc_ref.shape, f32)
    full = s // 2
    last = pl.multiple_of(full * KEYS, KEYS)

    def at(j):
        return pl.multiple_of(j * KEYS, KEYS)

    def before(j):
        return pl.multiple_of(jnp.where(j == 0, full, j - 1) * KEYS, KEYS)

    score(last, 0, s * ROWS - last)

    def body(t, carry):
        j = 2 * t
        score(at(j), 1, None)
        add(before(j), 0)
        score(at(j + 1), 0, None)
        add(at(j), 1)
        return carry

    lax.fori_loop(0, full // 2, body, 0)

    @pl.when(full % 2 == 1)
    def _():
        score(at(full - 1), 1, None)
        add(before(full - 1), 0)
        add(at(full - 1), 1)

    @pl.when(full % 2 == 0)
    def _():
        add(before(full), 0)

    for i, o_ref in enumerate((o0, o1, o2, o3)):

        @pl.when(step == i)
        def _():
            for h in range(PAIR):
                o_ref[h * 128 : (h + 1) * 128, :] = (acc_ref[h] / sum_ref[h]).astype(bf16)


def attend(yx, halves, cosine, sine, early):
    piece = jax.ShapeDtypeStruct((LOCAL * 128, ROWS), bf16)
    return pl.pallas_call(
        attend_kernel,
        grid=(LOCAL // PAIR, SIDE),
        in_specs=[SMEM] + [VMEM] * 12,
        out_specs=(pl.BlockSpec((PAIR * 128, ROWS), lambda h, i: (h, 0)),) * SIDE,
        out_shape=(piece,) * SIDE,
        scratch_shapes=[pltpu.VMEM(s, bf16) for s in EXPANDED]
        + [
            pltpu.VMEM((2, PAIR, KEYS, ROWS), f32),
            pltpu.VMEM((PAIR, 1, ROWS), f32),
            pltpu.VMEM((PAIR, 1, ROWS), f32),
            pltpu.VMEM((PAIR, 128, ROWS), f32),
        ],
        compiler_params=limit(32, dimension_semantics=("arbitrary", "arbitrary")),
        name="attend",
    )(yx, *halves, cosine, sine, *early)


WIDE = 512


def out_kernel(y_ref, p0, p1, p2, p3, w_ref, gain_ref, o_ref, rows_ref, proj_ref):
    y = y_ref[0]
    for i, piece in enumerate((p0, p1, p2, p3)):
        g = pl.multiple_of(((y + i) % 4) * 512, 512)
        rows_ref[:, pl.ds(g, 512)] = piece[...].T
    for n in range(0, 2048, WIDE):
        proj_ref[:, n : n + WIDE] = jnp.dot(
            rows_ref[...], w_ref[:, n : n + WIDE], preferred_element_type=f32
        )
    o_ref[...] = normed(proj_ref[...], gain_ref[...]).astype(bf16)


def project(y, pieces, w_out, gain):
    return pl.pallas_call(
        out_kernel,
        in_specs=[SMEM] + [VMEM] * 6,
        out_specs=VMEM,
        out_shape=jax.ShapeDtypeStruct((ROWS, 2048), bf16),
        scratch_shapes=[pltpu.VMEM((ROWS, 2048), bf16), pltpu.VMEM((ROWS, 2048), f32)],
        compiler_params=limit(16),
        name="project",
    )(y, *pieces, w_out, gain)


def stage_kernel(w_ref, o_ref, sem):
    copy = pltpu.make_async_copy(w_ref, o_ref, sem)
    copy.start()
    copy.wait()


def stage(w):
    return pl.pallas_call(
        stage_kernel,
        in_specs=[ANY],
        out_specs=VMEM,
        out_shape=jax.ShapeDtypeStruct(w.shape, w.dtype),
        scratch_shapes=[pltpu.SemaphoreType.DMA],
        compiler_params=limit(16),
        name="stage",
    )(w)


def up_columns(w_qup, w_kvup, y):
    rows = w_qup.shape[0]
    q = lax.dynamic_slice_in_dim(w_qup, y * LOCAL * 192, LOCAL * 192, 1).reshape(rows, LOCAL, 192)
    kv = lax.dynamic_slice_in_dim(w_kvup, y * LOCAL * 256, LOCAL * 256, 1).reshape(rows, LOCAL, 256)
    first = q[..., 128:160]
    second = q[..., 160:192]
    parts = [
        kv[..., :128],
        kv[..., 128:],
        q[..., :128],
        jnp.concatenate([first, second], axis=-1),
        jnp.concatenate([-second, first], axis=-1),
    ]
    return jnp.concatenate([p.reshape(rows, -1) for p in parts], axis=1)


def body(tokens, w_qdown, w_kvdown, w_rotary, q_gain, kv_gain, w_qup, w_kvup, w_out, out_gain):
    sp_place = lax.axis_index("sp")
    y = sp_place // SIDE
    x = sp_place % SIDE
    own = tokens[0]
    w_down = lax.all_gather(jnp.stack([w_kvdown, w_qdown]), "dp")

    lanes = jnp.arange(SIDE * 32)
    spots = ((y - lanes // 32 + SIDE) % SIDE) * SIDE + x
    positions = (spots[None, :] * ROWS + jnp.arange(ROWS)[:, None]).astype(f32)
    freqs = THETA ** (-(2 * (lanes % 32)).astype(f32) / ROPE)
    angles = positions * freqs[None, :]
    cosine = jnp.cos(angles)
    sine = jnp.sin(angles)

    turned = jnp.dot(own, w_rotary, preferred_element_type=f32)
    first = turned[:, :32]
    second = turned[:, 32:]
    cos_own = cosine[:, :32]
    sin_own = sine[:, :32]
    key_rot = jnp.concatenate(
        [first * cos_own - second * sin_own, second * cos_own + first * sin_own], axis=-1
    ).astype(bf16)
    packed = key_rot.reshape(2, 8, 16, 64).transpose(0, 2, 1, 3).reshape(2, 16, 512)

    w_own = z_blocks(up_columns(w_qup, w_kvup, y))
    w_other = lax.ppermute(w_own, "dp", PARTNER)
    dp_place = lax.axis_index("dp")
    yx = jnp.stack([y, x, dp_place // 2, dp_place % 2])
    w_down, w_own, w_other, cosine, sine, packed, yx = lax.optimization_barrier(
        (w_down, w_own, w_other, cosine, sine, packed, yx)
    )
    w_full = lax.all_gather(w_out, "dp", axis=1, tiled=True)

    gains = jnp.stack([kv_gain, q_gain]).reshape(2, 1, RANK)
    a, b, qn = down(own, w_down, gains, packed)

    b1, b2, b3 = (lax.ppermute(b, "sp", x_shift(k)) for k in (1, 2, 3))
    a1, a2, a3 = (lax.ppermute(a, "sp", y_shift(k)) for k in (1, 2, 3))
    col = jnp.concatenate([a, a1, a2, a3], axis=0)
    row = jnp.concatenate([b, b1, b2, b3, qn], axis=0)
    col1 = lax.ppermute(col, "sp", x_shift(1))
    col3 = lax.ppermute(col, "sp", x_shift(-1))
    row1 = lax.ppermute(row, "sp", y_shift(1))
    row3 = lax.ppermute(row, "sp", y_shift(-1))
    col2l = lax.ppermute(col1[:288], "sp", x_shift(1))
    col2h = lax.ppermute(col3[288:], "sp", x_shift(-1))
    row2l = lax.ppermute(row1[:416], "sp", y_shift(1))
    row2h = lax.ppermute(row3[416:], "sp", y_shift(-1))

    early = expand_early(
        yx, (col, col1, col3, row, row1, row3), w_own, w_other, cosine, sine
    )
    attended = attend(yx, (col2l, col2h, row2l, row2h), cosine, sine, early)
    w_full, *attended = lax.optimization_barrier((w_full, *attended))
    pieces = [attended[0]] + [
        lax.ppermute(attended[i], "sp", y_shift(-i)) for i in range(1, SIDE)
    ]
    mixed = project(y.reshape(1), pieces, stage(w_full), out_gain.reshape(1, 2048))
    return mixed[None]


def solution(mesh):
    in_specs = (
        P("dp", "sp", None),
        P("dp", None),
        P("dp", None),
        P(),
        P(),
        P(),
        P("dp", None),
        P("dp", None),
        P(None, "dp"),
        P(),
    )
    out_specs = P("dp", "sp", None)

    return jax.shard_map(body, mesh=mesh, in_specs=in_specs, out_specs=out_specs, check_vma=False)
```

```python
import jax
import jax.numpy as jnp
from jax import lax
from jax.experimental import pallas as pl
from jax.experimental.pallas import tpu as pltpu
from jax.sharding import PartitionSpec as P


HEADS = 16
NOPE = 128
ROPE = 64
RANK = 512
ROWS = 256
SIDE = 4
LENGTH = 4096
LOCAL = HEADS // SIDE
PIECE = 144

EPSILON = 1e-06
THETA = 10000.0
LOG2E = 1.4426950408889634
SCALE2 = (NOPE + ROPE) ** (-0.5) * LOG2E
MIB = 2**20


f32 = jnp.float32
bf16 = jnp.bfloat16


PARTNER = [(d, d ^ 1) for d in range(16)]


def z_shift(k):
    return [(d, (d + 2 * k) % 16) for d in range(16)]


def z_blocks(w):
    blocks = [w] + [None] * 7
    ahead = behind = w
    for i in range(1, 4):
        ahead = lax.ppermute(ahead, "dp", z_shift(1))
        behind = lax.ppermute(behind, "dp", z_shift(-1))
        blocks[i] = ahead
        blocks[8 - i] = behind
    blocks[4] = lax.ppermute(ahead, "dp", z_shift(1))
    return jnp.concatenate(blocks, axis=0)


def y_shift(k):
    return [(s, (s + SIDE * k) % 16) for s in range(16)]


def x_shift(k):
    return [(s, (s // SIDE) * SIDE + (s % SIDE + k) % SIDE) for s in range(16)]


def limit(mib, **kw):
    return pltpu.CompilerParams(vmem_limit_bytes=mib * MIB, **kw)


SMEM = pl.BlockSpec(memory_space=pltpu.SMEM)
VMEM = pl.BlockSpec(memory_space=pltpu.VMEM)
ANY = pl.BlockSpec(memory_space=pl.ANY)


def normed(values, gain):
    scale = lax.rsqrt(jnp.mean(values * values, axis=-1, keepdims=True) + EPSILON)
    return values * scale * gain


def down_kernel(rows_ref, w_ref, gain_ref, rot_ref, a_ref, b_ref, q_ref):
    w = w_ref[...].reshape(2048, RANK)
    lat = jnp.dot(rows_ref[...], w, preferred_element_type=f32)
    lat = normed(lat, gain_ref[0]).astype(bf16)

    @pl.when(pl.program_id(0) == 0)
    def _():
        a_ref[0:128, :] = lat[0:128]
        a_ref[128:PIECE, :] = rot_ref[0]
        b_ref[0:128, :] = lat[128:256]
        b_ref[128:PIECE, :] = rot_ref[1]

    @pl.when(pl.program_id(0) == 1)
    def _():
        q_ref[...] = lat


def down(rows, w, gains, rot):
    piece = jax.ShapeDtypeStruct((PIECE, RANK), bf16)
    return pl.pallas_call(
        down_kernel,
        grid=(2,),
        in_specs=[
            pl.BlockSpec((ROWS, 2048), lambda n: (0, 0)),
            pl.BlockSpec((16, 1, 128, RANK), lambda n: (0, n, 0, 0)),
            pl.BlockSpec((1, 1, RANK), lambda n: (n, 0, 0)),
            pl.BlockSpec((2, 16, RANK), lambda n: (0, 0, 0)),
        ],
        out_specs=(
            pl.BlockSpec((PIECE, RANK), lambda n: (0, 0)),
            pl.BlockSpec((PIECE, RANK), lambda n: (0, 0)),
            pl.BlockSpec((ROWS, RANK), lambda n: (0, 0)),
        ),
        out_shape=(piece, piece, jax.ShapeDtypeStruct((ROWS, RANK), bf16)),
        compiler_params=limit(60, dimension_semantics=("arbitrary",)),
        name="down",
    )(rows, w, gains, rot)


def reader(low, high=None):
    def read(at, count):
        cut = low.shape[0]
        if at < cut:
            return low[at : at + count, :]
        return high[at - cut : at - cut + count, :]

    return read


def spot(yx_ref, i, j, half):
    at = ((yx_ref[0] - i + 4) % 4 * 4 + (yx_ref[1] - j + 4) % 4) * 256 + half * 128
    return pl.multiple_of(at, 128)


def expand(read, spots, w_ref, wvt_ref, k_ref, r_ref, vt_ref):
    rows = jnp.concatenate([read(PIECE * n, 128) for n in range(4)], axis=0)
    keys = jnp.dot(rows, w_ref[:, 0:512], preferred_element_type=f32).astype(bf16)
    values = lax.dot_general(
        wvt_ref[...], rows, (((1,), (1,)), ((), ())), preferred_element_type=f32
    ).astype(bf16)
    for n, at in enumerate(spots):
        for p in range(2):
            k_ref[p, pl.ds(at, 128), :] = keys[128 * n : 128 * n + 128, 256 * p : 256 * p + 256]
            vt_ref[p, :, pl.ds(at, 128)] = values[256 * p : 256 * p + 256, 128 * n : 128 * n + 128]
        packed = read(PIECE * n + 128, 16)
        rot = jnp.concatenate([packed[:, 64 * u : 64 * u + 64] for u in range(8)], axis=0)
        r_ref[pl.ds(at, 128), :] = jnp.concatenate([rot, jnp.zeros((128, 64), bf16)], axis=1)


def expand_queries(qn, i, w_ref, cos_ref, sin_ref, q_ref):
    both = jnp.dot(qn, w_ref[:, 1024:2048], preferred_element_type=f32)
    cosine = jnp.concatenate([cos_ref[:, 32 * i : 32 * i + 32]] * 8, axis=1)
    sine = jnp.concatenate([sin_ref[:, 32 * i : 32 * i + 32]] * 8, axis=1)
    turned = (both[:, 512:768] * cosine + both[:, 768:1024] * sine).astype(bf16)
    pad = jnp.zeros((ROWS, 64), bf16)
    for h in range(LOCAL):
        q_ref[h, ROWS * i : ROWS * (i + 1), 0:128] = both[:, 128 * h : 128 * h + 128].astype(bf16)
        q_ref[h, ROWS * i : ROWS * (i + 1), 128:256] = jnp.concatenate(
            [turned[:, 64 * h : 64 * h + 64], pad], axis=1
        )


COL = 4 * PIECE
ROW = COL + ROWS
UP = 32


def early_kernel(
    yx_ref, a0, a1, a3, b0, b1, b3, own_w, other_w, cos_ref, sin_ref,
    k_ref, r_ref, vt_ref, q_ref, w_ref, wvt_ref,
):
    z = yx_ref[2]
    core = yx_ref[3]
    for i in range(8):
        at = ((z - i + 8) % 8) * 2 * UP
        for ref, part in ((own_w, core), (other_w, 1 - core)):
            spot_at = pl.multiple_of(at + part * UP, UP)
            w_ref[pl.ds(spot_at, UP), :] = ref[UP * i : UP * (i + 1), :]
    wvt_ref[...] = w_ref[:, 512:1024].T
    outs = (w_ref, wvt_ref, k_ref, r_ref, vt_ref)
    for j, piece in ((0, a0), (1, a1), (3, a3)):
        expand(reader(piece), [spot(yx_ref, i, j, 0) for i in range(4)], *outs)
    for i, piece in ((0, b0), (1, b1), (3, b3)):
        expand(reader(piece), [spot(yx_ref, i, j, 1) for j in range(4)], *outs)
        expand_queries(piece[COL:ROW, :], i, w_ref, cos_ref, sin_ref, q_ref)


EXPANDED = (
    (2, LENGTH, 256),
    (LENGTH, 128),
    (2, 256, LENGTH),
    (LOCAL, SIDE * ROWS, 256),
)


def expand_early(yx, parts, w_own, w_other, cosine, sine):
    out = EXPANDED + ((RANK, 2048), (512, RANK))
    return pl.pallas_call(
        early_kernel,
        out_shape=tuple(jax.ShapeDtypeStruct(s, bf16) for s in out),
        in_specs=[SMEM] + [VMEM] * 10,
        out_specs=(VMEM,) * 6,
        compiler_params=limit(20),
        name="early",
    )(yx, *parts, w_own, w_other, cosine, sine)


KEYS = 512
PAIR = 2


def attend_kernel(
    yx_ref, a2l, a2h, b2l, b2h, cos_ref, sin_ref, k_in, r_in, vt_in, q_in, w_ref, wvt_ref,
    o0, o1, o2, o3, k_ref, r_ref, vt_ref, q_ref, score_ref, top_ref, sum_ref, acc_ref,
):
    pair = pl.program_id(0)
    step = pl.program_id(1)

    @pl.when((pair == 0) & (step == 0))
    def _():
        for p in range(2):
            k_ref[p] = k_in[p]
            vt_ref[p] = vt_in[p]
        r_ref[...] = r_in[...]
        for h in range(LOCAL):
            q_ref[h] = q_in[h]
        outs = (w_ref, wvt_ref, k_ref, r_ref, vt_ref)
        expand(reader(a2l, a2h), [spot(yx_ref, i, 2, 0) for i in range(4)], *outs)
        last = reader(b2l, b2h)
        expand(last, [spot(yx_ref, 2, j, 1) for j in range(4)], *outs)
        expand_queries(last(4 * PIECE, ROWS), 2, w_ref, cos_ref, sin_ref, q_ref)

    s = (yx_ref[0] - step + 4) % 4 * 4 + yx_ref[1]
    mine = pl.multiple_of(step * ROWS, ROWS)

    def score(at, slot, ahead):
        rot = r_ref[pl.ds(at, KEYS), :]
        for h in range(PAIR):
            keys = jnp.concatenate([k_ref[pair, pl.ds(at, KEYS), 128 * h : 128 * h + 128], rot], axis=1)
            query = q_ref[PAIR * pair + h, pl.ds(mine, ROWS), :]
            st = lax.dot_general(keys, query, (((1,), (1,)), ((), ())), preferred_element_type=f32)
            if ahead is not None:
                key_pos = lax.broadcasted_iota(jnp.int32, st.shape, 0)
                query_pos = lax.broadcasted_iota(jnp.int32, st.shape, 1)
                st = jnp.where(key_pos <= query_pos + ahead, st, -jnp.inf)
            score_ref[slot, h] = st

    def add(at, slot):
        for h in range(PAIR):
            st = score_ref[slot, h]
            top = top_ref[h]
            new = jnp.maximum(top, jnp.max(st, axis=0, keepdims=True))
            expo = jnp.exp2(st * SCALE2 - new * SCALE2)
            fade = jnp.exp2((top - new) * SCALE2)
            top_ref[h] = new
            sum_ref[h] = sum_ref[h] * fade + jnp.sum(expo, axis=0, keepdims=True)
            acc_ref[h] = acc_ref[h] * fade + jnp.dot(
                vt_ref[pair, 128 * h : 128 * h + 128, pl.ds(at, KEYS)],
                expo.astype(bf16),
                preferred_element_type=f32,
            )

    top_ref[...] = jnp.full(top_ref.shape, -jnp.inf, f32)
    sum_ref[...] = jnp.zeros(sum_ref.shape, f32)
    acc_ref[...] = jnp.zeros(acc_ref.shape, f32)
    full = s // 2
    last = pl.multiple_of(full * KEYS, KEYS)

    def at(j):
        return pl.multiple_of(j * KEYS, KEYS)

    def before(j):
        return pl.multiple_of(jnp.where(j == 0, full, j - 1) * KEYS, KEYS)

    score(last, 0, s * ROWS - last)

    def body(t, carry):
        j = 2 * t
        score(at(j), 1, None)
        add(before(j), 0)
        score(at(j + 1), 0, None)
        add(at(j), 1)
        return carry

    lax.fori_loop(0, full // 2, body, 0)

    @pl.when(full % 2 == 1)
    def _():
        score(at(full - 1), 1, None)
        add(before(full - 1), 0)
        add(at(full - 1), 1)

    @pl.when(full % 2 == 0)
    def _():
        add(before(full), 0)

    for i, o_ref in enumerate((o0, o1, o2, o3)):

        @pl.when(step == i)
        def _():
            for h in range(PAIR):
                o_ref[h * 128 : (h + 1) * 128, :] = (acc_ref[h] / sum_ref[h]).astype(bf16)


def attend(yx, halves, cosine, sine, early):
    piece = jax.ShapeDtypeStruct((LOCAL * 128, ROWS), bf16)
    return pl.pallas_call(
        attend_kernel,
        grid=(LOCAL // PAIR, SIDE),
        in_specs=[SMEM] + [VMEM] * 12,
        out_specs=(pl.BlockSpec((PAIR * 128, ROWS), lambda h, i: (h, 0)),) * SIDE,
        out_shape=(piece,) * SIDE,
        scratch_shapes=[pltpu.VMEM(s, bf16) for s in EXPANDED]
        + [
            pltpu.VMEM((2, PAIR, KEYS, ROWS), f32),
            pltpu.VMEM((PAIR, 1, ROWS), f32),
            pltpu.VMEM((PAIR, 1, ROWS), f32),
            pltpu.VMEM((PAIR, 128, ROWS), f32),
        ],
        compiler_params=limit(32, dimension_semantics=("arbitrary", "arbitrary")),
        name="attend",
    )(yx, *halves, cosine, sine, *early)


WIDE = 512


def out_kernel(y_ref, p0, p1, p2, p3, w_ref, gain_ref, o_ref, rows_ref, proj_ref):
    y = y_ref[0]
    for i, piece in enumerate((p0, p1, p2, p3)):
        g = pl.multiple_of(((y + i) % 4) * 512, 512)
        rows_ref[:, pl.ds(g, 512)] = piece[...].T
    for n in range(0, 2048, WIDE):
        proj_ref[:, n : n + WIDE] = jnp.dot(
            rows_ref[...], w_ref[:, n : n + WIDE], preferred_element_type=f32
        )
    o_ref[...] = normed(proj_ref[...], gain_ref[...]).astype(bf16)


def project(y, pieces, w_out, gain):
    return pl.pallas_call(
        out_kernel,
        in_specs=[SMEM] + [VMEM] * 6,
        out_specs=VMEM,
        out_shape=jax.ShapeDtypeStruct((ROWS, 2048), bf16),
        scratch_shapes=[pltpu.VMEM((ROWS, 2048), bf16), pltpu.VMEM((ROWS, 2048), f32)],
        compiler_params=limit(16),
        name="project",
    )(y, *pieces, w_out, gain)


def stage_kernel(w_ref, o_ref, sem):
    copy = pltpu.make_async_copy(w_ref, o_ref, sem)
    copy.start()
    copy.wait()


def stage(w):
    return pl.pallas_call(
        stage_kernel,
        in_specs=[ANY],
        out_specs=VMEM,
        out_shape=jax.ShapeDtypeStruct(w.shape, w.dtype),
        scratch_shapes=[pltpu.SemaphoreType.DMA],
        compiler_params=limit(16),
        name="stage",
    )(w)


def up_columns(w_qup, w_kvup, y):
    rows = w_qup.shape[0]
    q = lax.dynamic_slice_in_dim(w_qup, y * LOCAL * 192, LOCAL * 192, 1).reshape(rows, LOCAL, 192)
    kv = lax.dynamic_slice_in_dim(w_kvup, y * LOCAL * 256, LOCAL * 256, 1).reshape(rows, LOCAL, 256)
    first = q[..., 128:160]
    second = q[..., 160:192]
    parts = [
        kv[..., :128],
        kv[..., 128:],
        q[..., :128],
        jnp.concatenate([first, second], axis=-1),
        jnp.concatenate([-second, first], axis=-1),
    ]
    return jnp.concatenate([p.reshape(rows, -1) for p in parts], axis=1)


def body(tokens, w_qdown, w_kvdown, w_rotary, q_gain, kv_gain, w_qup, w_kvup, w_out, out_gain):
    sp_place = lax.axis_index("sp")
    y = sp_place // SIDE
    x = sp_place % SIDE
    own = tokens[0]
    w_down = lax.all_gather(jnp.stack([w_kvdown, w_qdown]), "dp")

    lanes = jnp.arange(SIDE * 32)
    spots = ((y - lanes // 32 + SIDE) % SIDE) * SIDE + x
    positions = (spots[None, :] * ROWS + jnp.arange(ROWS)[:, None]).astype(f32)
    freqs = THETA ** (-(2 * (lanes % 32)).astype(f32) / ROPE)
    angles = positions * freqs[None, :]
    cosine = jnp.cos(angles)
    sine = jnp.sin(angles)

    turned = jnp.dot(own, w_rotary, preferred_element_type=f32)
    first = turned[:, :32]
    second = turned[:, 32:]
    cos_own = cosine[:, :32]
    sin_own = sine[:, :32]
    key_rot = jnp.concatenate(
        [first * cos_own - second * sin_own, second * cos_own + first * sin_own], axis=-1
    ).astype(bf16)
    packed = key_rot.reshape(2, 8, 16, 64).transpose(0, 2, 1, 3).reshape(2, 16, 512)

    w_own = z_blocks(up_columns(w_qup, w_kvup, y))
    w_other = lax.ppermute(w_own, "dp", PARTNER)
    dp_place = lax.axis_index("dp")
    yx = jnp.stack([y, x, dp_place // 2, dp_place % 2])
    w_down, w_own, w_other, cosine, sine, packed, yx = lax.optimization_barrier(
        (w_down, w_own, w_other, cosine, sine, packed, yx)
    )
    w_full = lax.all_gather(w_out, "dp", axis=1, tiled=True)

    gains = jnp.stack([kv_gain, q_gain]).reshape(2, 1, RANK)
    a, b, qn = down(own, w_down, gains, packed)

    b1, b2, b3 = (lax.ppermute(b, "sp", x_shift(k)) for k in (1, 2, 3))
    a1, a2, a3 = (lax.ppermute(a, "sp", y_shift(k)) for k in (1, 2, 3))
    col = jnp.concatenate([a, a1, a2, a3], axis=0)
    row = jnp.concatenate([b, b1, b2, b3, qn], axis=0)
    col1 = lax.ppermute(col, "sp", x_shift(1))
    col3 = lax.ppermute(col, "sp", x_shift(-1))
    row1 = lax.ppermute(row, "sp", y_shift(1))
    row3 = lax.ppermute(row, "sp", y_shift(-1))
    col2l = lax.ppermute(col1[:288], "sp", x_shift(1))
    col2h = lax.ppermute(col3[288:], "sp", x_shift(-1))
    row2l = lax.ppermute(row1[:416], "sp", y_shift(1))
    row2h = lax.ppermute(row3[416:], "sp", y_shift(-1))

    early = expand_early(
        yx, (col, col1, col3, row, row1, row3), w_own, w_other, cosine, sine
    )
    attended = attend(yx, (col2l, col2h, row2l, row2h), cosine, sine, early)
    w_full, *attended = lax.optimization_barrier((w_full, *attended))
    pieces = [attended[0]] + [
        lax.ppermute(attended[i], "sp", y_shift(-i)) for i in range(1, SIDE)
    ]
    mixed = project(y.reshape(1), pieces, stage(w_full), out_gain.reshape(1, 2048))
    return mixed[None]


def solution(mesh):
    in_specs = (
        P("dp", "sp", None),
        P("dp", None),
        P("dp", None),
        P(),
        P(),
        P(),
        P("dp", None),
        P("dp", None),
        P(None, "dp"),
        P(),
    )
    out_specs = P("dp", "sp", None)

    return jax.shard_map(body, mesh=mesh, in_specs=in_specs, out_specs=out_specs, check_vma=False)
```

```python
import jax
import jax.numpy as jnp
from jax import lax
from jax.experimental import pallas as pl
from jax.experimental.pallas import tpu as pltpu
from jax.sharding import PartitionSpec as P


HEADS = 16
NOPE = 128
ROPE = 64
RANK = 512
ROWS = 256
SIDE = 4
LENGTH = 4096
LOCAL = HEADS // SIDE
PIECE = 144

EPSILON = 1e-06
THETA = 10000.0
LOG2E = 1.4426950408889634
SCALE2 = (NOPE + ROPE) ** (-0.5) * LOG2E
MIB = 2**20


f32 = jnp.float32
bf16 = jnp.bfloat16


PARTNER = [(d, d ^ 1) for d in range(16)]


def z_shift(k):
    return [(d, (d + 2 * k) % 16) for d in range(16)]


def z_blocks(w):
    blocks = [w] + [None] * 7
    ahead = behind = w
    for i in range(1, 4):
        ahead = lax.ppermute(ahead, "dp", z_shift(1))
        behind = lax.ppermute(behind, "dp", z_shift(-1))
        blocks[i] = ahead
        blocks[8 - i] = behind
    blocks[4] = lax.ppermute(ahead, "dp", z_shift(1))
    return jnp.concatenate(blocks, axis=0)


def y_shift(k):
    return [(s, (s + SIDE * k) % 16) for s in range(16)]


def x_shift(k):
    return [(s, (s // SIDE) * SIDE + (s % SIDE + k) % SIDE) for s in range(16)]


def limit(mib, **kw):
    return pltpu.CompilerParams(vmem_limit_bytes=mib * MIB, **kw)


SMEM = pl.BlockSpec(memory_space=pltpu.SMEM)
VMEM = pl.BlockSpec(memory_space=pltpu.VMEM)
ANY = pl.BlockSpec(memory_space=pl.ANY)


def normed(values, gain):
    scale = lax.rsqrt(jnp.mean(values * values, axis=-1, keepdims=True) + EPSILON)
    return values * scale * gain


def latent(rows_ref, w_ref, gain_ref):
    w = w_ref[...].reshape(2048, RANK)
    lat = jnp.dot(rows_ref[...], w, preferred_element_type=f32)
    return normed(lat, gain_ref[...]).astype(bf16)


def kv_down_kernel(rows_ref, w_ref, gain_ref, rot_ref, a_ref, b_ref):
    lat = latent(rows_ref, w_ref, gain_ref)
    a_ref[0:128, :] = lat[0:128]
    a_ref[128:PIECE, :] = rot_ref[0]
    b_ref[0:128, :] = lat[128:256]
    b_ref[128:PIECE, :] = rot_ref[1]


def q_down_kernel(rows_ref, w_ref, gain_ref, q_ref):
    q_ref[...] = latent(rows_ref, w_ref, gain_ref)


def down(kernel, which, out, rows, w, gain, *rot):
    def whole(shape):
        return pl.BlockSpec(shape, lambda n: (0,) * len(shape))

    return pl.pallas_call(
        kernel,
        grid=(1,),
        in_specs=[
            whole(rows.shape),
            pl.BlockSpec((16, 1, 128, RANK), lambda n: (0, which, 0, 0)),
            whole(gain.shape),
        ]
        + [whole(r.shape) for r in rot],
        out_specs=tuple(whole(shape) for shape in out),
        out_shape=tuple(jax.ShapeDtypeStruct(shape, bf16) for shape in out),
        compiler_params=limit(60, dimension_semantics=("arbitrary",)),
        name="down",
    )(rows, w, gain, *rot)


def reader(low, high=None):
    def read(at, count):
        cut = low.shape[0]
        if at < cut:
            return low[at : at + count, :]
        return high[at - cut : at - cut + count, :]

    return read


def spot(yx_ref, i, j, half):
    at = ((yx_ref[0] - i + 4) % 4 * 4 + (yx_ref[1] - j + 4) % 4) * 256 + half * 128
    return pl.multiple_of(at, 128)


def expand(read, spots, w_ref, wvt_ref, k_ref, r_ref, vt_ref):
    rows = jnp.concatenate([read(PIECE * n, 128) for n in range(4)], axis=0)
    keys = jnp.dot(rows, w_ref[:, 0:512], preferred_element_type=f32).astype(bf16)
    values = lax.dot_general(
        wvt_ref[...], rows, (((1,), (1,)), ((), ())), preferred_element_type=f32
    ).astype(bf16)
    for n, at in enumerate(spots):
        for p in range(2):
            k_ref[p, pl.ds(at, 128), :] = keys[128 * n : 128 * n + 128, 256 * p : 256 * p + 256]
            vt_ref[p, :, pl.ds(at, 128)] = values[256 * p : 256 * p + 256, 128 * n : 128 * n + 128]
        packed = read(PIECE * n + 128, 16)
        rot = jnp.concatenate([packed[:, 64 * u : 64 * u + 64] for u in range(8)], axis=0)
        r_ref[pl.ds(at, 128), :] = jnp.concatenate([rot, jnp.zeros((128, 64), bf16)], axis=1)


def expand_queries(qn, i, w_ref, cos_ref, sin_ref, q_ref):
    both = jnp.dot(qn, w_ref[:, 1024:2048], preferred_element_type=f32)
    cosine = jnp.concatenate([cos_ref[:, 32 * i : 32 * i + 32]] * 8, axis=1)
    sine = jnp.concatenate([sin_ref[:, 32 * i : 32 * i + 32]] * 8, axis=1)
    turned = (both[:, 512:768] * cosine + both[:, 768:1024] * sine).astype(bf16)
    pad = jnp.zeros((ROWS, 64), bf16)
    for h in range(LOCAL):
        q_ref[h, ROWS * i : ROWS * (i + 1), 0:128] = both[:, 128 * h : 128 * h + 128].astype(bf16)
        q_ref[h, ROWS * i : ROWS * (i + 1), 128:256] = jnp.concatenate(
            [turned[:, 64 * h : 64 * h + 64], pad], axis=1
        )


COL = 4 * PIECE
ROW = COL + ROWS
UP = 32


def early_kernel(
    yx_ref, a0, a1, a3, b0, b1, b3, own_w, other_w, cos_ref, sin_ref,
    k_ref, r_ref, vt_ref, q_ref, w_ref, wvt_ref,
):
    z = yx_ref[2]
    core = yx_ref[3]
    for i in range(8):
        at = ((z - i + 8) % 8) * 2 * UP
        for ref, part in ((own_w, core), (other_w, 1 - core)):
            spot_at = pl.multiple_of(at + part * UP, UP)
            w_ref[pl.ds(spot_at, UP), :] = ref[UP * i : UP * (i + 1), :]
    wvt_ref[...] = w_ref[:, 512:1024].T
    outs = (w_ref, wvt_ref, k_ref, r_ref, vt_ref)
    for j, piece in ((0, a0), (1, a1), (3, a3)):
        expand(reader(piece), [spot(yx_ref, i, j, 0) for i in range(4)], *outs)
    for i, piece in ((0, b0), (1, b1), (3, b3)):
        expand(reader(piece), [spot(yx_ref, i, j, 1) for j in range(4)], *outs)
        expand_queries(piece[COL:ROW, :], i, w_ref, cos_ref, sin_ref, q_ref)


EXPANDED = (
    (2, LENGTH, 256),
    (LENGTH, 128),
    (2, 256, LENGTH),
    (LOCAL, SIDE * ROWS, 256),
)


def expand_early(yx, parts, w_own, w_other, cosine, sine):
    out = EXPANDED + ((RANK, 2048), (512, RANK))
    return pl.pallas_call(
        early_kernel,
        out_shape=tuple(jax.ShapeDtypeStruct(s, bf16) for s in out),
        in_specs=[SMEM] + [VMEM] * 10,
        out_specs=(VMEM,) * 6,
        compiler_params=limit(20),
        name="early",
    )(yx, *parts, w_own, w_other, cosine, sine)


KEYS = 512
PAIR = 2


def attend_kernel(
    yx_ref, a2l, a2h, b2l, b2h, cos_ref, sin_ref, k_in, r_in, vt_in, q_in, w_ref, wvt_ref,
    o0, o1, o2, o3, k_ref, r_ref, vt_ref, q_ref, score_ref, top_ref, sum_ref, acc_ref,
):
    pair = pl.program_id(0)
    step = pl.program_id(1)

    @pl.when((pair == 0) & (step == 0))
    def _():
        for p in range(2):
            k_ref[p] = k_in[p]
            vt_ref[p] = vt_in[p]
        r_ref[...] = r_in[...]
        for h in range(LOCAL):
            q_ref[h] = q_in[h]
        outs = (w_ref, wvt_ref, k_ref, r_ref, vt_ref)
        expand(reader(a2l, a2h), [spot(yx_ref, i, 2, 0) for i in range(4)], *outs)
        last = reader(b2l, b2h)
        expand(last, [spot(yx_ref, 2, j, 1) for j in range(4)], *outs)
        expand_queries(last(4 * PIECE, ROWS), 2, w_ref, cos_ref, sin_ref, q_ref)

    s = (yx_ref[0] - step + 4) % 4 * 4 + yx_ref[1]
    mine = pl.multiple_of(step * ROWS, ROWS)

    def score(at, slot, ahead):
        rot = r_ref[pl.ds(at, KEYS), :]
        for h in range(PAIR):
            keys = jnp.concatenate([k_ref[pair, pl.ds(at, KEYS), 128 * h : 128 * h + 128], rot], axis=1)
            query = q_ref[PAIR * pair + h, pl.ds(mine, ROWS), :]
            st = lax.dot_general(keys, query, (((1,), (1,)), ((), ())), preferred_element_type=f32)
            if ahead is not None:
                key_pos = lax.broadcasted_iota(jnp.int32, st.shape, 0)
                query_pos = lax.broadcasted_iota(jnp.int32, st.shape, 1)
                st = jnp.where(key_pos <= query_pos + ahead, st, -jnp.inf)
            score_ref[slot, h] = st

    def add(at, slot):
        for h in range(PAIR):
            st = score_ref[slot, h]
            top = top_ref[h]
            new = jnp.maximum(top, jnp.max(st, axis=0, keepdims=True))
            expo = jnp.exp2(st * SCALE2 - new * SCALE2)
            fade = jnp.exp2((top - new) * SCALE2)
            top_ref[h] = new
            sum_ref[h] = sum_ref[h] * fade + jnp.sum(expo, axis=0, keepdims=True)
            acc_ref[h] = acc_ref[h] * fade + jnp.dot(
                vt_ref[pair, 128 * h : 128 * h + 128, pl.ds(at, KEYS)],
                expo.astype(bf16),
                preferred_element_type=f32,
            )

    top_ref[...] = jnp.full(top_ref.shape, -jnp.inf, f32)
    sum_ref[...] = jnp.zeros(sum_ref.shape, f32)
    acc_ref[...] = jnp.zeros(acc_ref.shape, f32)
    full = s // 2
    last = pl.multiple_of(full * KEYS, KEYS)

    def at(j):
        return pl.multiple_of(j * KEYS, KEYS)

    def before(j):
        return pl.multiple_of(jnp.where(j == 0, full, j - 1) * KEYS, KEYS)

    score(last, 0, s * ROWS - last)

    def body(t, carry):
        j = 2 * t
        score(at(j), 1, None)
        add(before(j), 0)
        score(at(j + 1), 0, None)
        add(at(j), 1)
        return carry

    lax.fori_loop(0, full // 2, body, 0)

    @pl.when(full % 2 == 1)
    def _():
        score(at(full - 1), 1, None)
        add(before(full - 1), 0)
        add(at(full - 1), 1)

    @pl.when(full % 2 == 0)
    def _():
        add(before(full), 0)

    for i, o_ref in enumerate((o0, o1, o2, o3)):

        @pl.when(step == i)
        def _():
            for h in range(PAIR):
                o_ref[h * 128 : (h + 1) * 128, :] = (acc_ref[h] / sum_ref[h]).astype(bf16)


def attend(yx, halves, cosine, sine, early):
    piece = jax.ShapeDtypeStruct((LOCAL * 128, ROWS), bf16)
    return pl.pallas_call(
        attend_kernel,
        grid=(LOCAL // PAIR, SIDE),
        in_specs=[SMEM] + [VMEM] * 12,
        out_specs=(pl.BlockSpec((PAIR * 128, ROWS), lambda h, i: (h, 0)),) * SIDE,
        out_shape=(piece,) * SIDE,
        scratch_shapes=[pltpu.VMEM(s, bf16) for s in EXPANDED]
        + [
            pltpu.VMEM((2, PAIR, KEYS, ROWS), f32),
            pltpu.VMEM((PAIR, 1, ROWS), f32),
            pltpu.VMEM((PAIR, 1, ROWS), f32),
            pltpu.VMEM((PAIR, 128, ROWS), f32),
        ],
        compiler_params=limit(32, dimension_semantics=("arbitrary", "arbitrary")),
        name="attend",
    )(yx, *halves, cosine, sine, *early)


WIDE = 512


def out_kernel(y_ref, p0, p1, p2, p3, w_ref, gain_ref, o_ref, rows_ref, proj_ref):
    y = y_ref[0]
    for i, piece in enumerate((p0, p1, p2, p3)):
        g = pl.multiple_of(((y + i) % 4) * 512, 512)
        rows_ref[:, pl.ds(g, 512)] = piece[...].T
    for n in range(0, 2048, WIDE):
        proj_ref[:, n : n + WIDE] = jnp.dot(
            rows_ref[...], w_ref[:, n : n + WIDE], preferred_element_type=f32
        )
    o_ref[...] = normed(proj_ref[...], gain_ref[...]).astype(bf16)


def project(y, pieces, w_out, gain):
    return pl.pallas_call(
        out_kernel,
        in_specs=[SMEM] + [VMEM] * 6,
        out_specs=VMEM,
        out_shape=jax.ShapeDtypeStruct((ROWS, 2048), bf16),
        scratch_shapes=[pltpu.VMEM((ROWS, 2048), bf16), pltpu.VMEM((ROWS, 2048), f32)],
        compiler_params=limit(16),
        name="project",
    )(y, *pieces, w_out, gain)


def stage_kernel(w_ref, o_ref, sem):
    copy = pltpu.make_async_copy(w_ref, o_ref, sem)
    copy.start()
    copy.wait()


def stage(w):
    return pl.pallas_call(
        stage_kernel,
        in_specs=[ANY],
        out_specs=VMEM,
        out_shape=jax.ShapeDtypeStruct(w.shape, w.dtype),
        scratch_shapes=[pltpu.SemaphoreType.DMA],
        compiler_params=limit(16),
        name="stage",
    )(w)


def up_columns(w_qup, w_kvup, y):
    rows = w_qup.shape[0]
    q = lax.dynamic_slice_in_dim(w_qup, y * LOCAL * 192, LOCAL * 192, 1).reshape(rows, LOCAL, 192)
    kv = lax.dynamic_slice_in_dim(w_kvup, y * LOCAL * 256, LOCAL * 256, 1).reshape(rows, LOCAL, 256)
    first = q[..., 128:160]
    second = q[..., 160:192]
    parts = [
        kv[..., :128],
        kv[..., 128:],
        q[..., :128],
        jnp.concatenate([first, second], axis=-1),
        jnp.concatenate([-second, first], axis=-1),
    ]
    return jnp.concatenate([p.reshape(rows, -1) for p in parts], axis=1)


def body(tokens, w_qdown, w_kvdown, w_rotary, q_gain, kv_gain, w_qup, w_kvup, w_out, out_gain):
    sp_place = lax.axis_index("sp")
    y = sp_place // SIDE
    x = sp_place % SIDE
    own = tokens[0]
    w_down = lax.all_gather(jnp.stack([w_kvdown, w_qdown]), "dp")

    lanes = jnp.arange(SIDE * 32)
    spots = ((y - lanes // 32 + SIDE) % SIDE) * SIDE + x
    positions = (spots[None, :] * ROWS + jnp.arange(ROWS)[:, None]).astype(f32)
    freqs = THETA ** (-(2 * (lanes % 32)).astype(f32) / ROPE)
    angles = positions * freqs[None, :]
    cosine = jnp.cos(angles)
    sine = jnp.sin(angles)

    turned = jnp.dot(own, w_rotary, preferred_element_type=f32)
    first = turned[:, :32]
    second = turned[:, 32:]
    cos_own = cosine[:, :32]
    sin_own = sine[:, :32]
    key_rot = jnp.concatenate(
        [first * cos_own - second * sin_own, second * cos_own + first * sin_own], axis=-1
    ).astype(bf16)
    packed = key_rot.reshape(2, 8, 16, 64).transpose(0, 2, 1, 3).reshape(2, 16, 512)

    w_own = z_blocks(up_columns(w_qup, w_kvup, y))
    w_other = lax.ppermute(w_own, "dp", PARTNER)
    dp_place = lax.axis_index("dp")
    yx = jnp.stack([y, x, dp_place // 2, dp_place % 2])
    w_down, w_own, w_other, cosine, sine, packed, yx = lax.optimization_barrier(
        (w_down, w_own, w_other, cosine, sine, packed, yx)
    )
    w_full = lax.all_gather(w_out, "dp", axis=1, tiled=True)

    gain = kv_gain.reshape(1, RANK)
    a, b = down(kv_down_kernel, 0, ((PIECE, RANK),) * 2, own, w_down, gain, packed)
    (qn,) = down(q_down_kernel, 1, ((ROWS, RANK),), own, w_down, q_gain.reshape(1, RANK))

    b1, b2, b3 = (lax.ppermute(b, "sp", x_shift(k)) for k in (1, 2, 3))
    a1, a2, a3 = (lax.ppermute(a, "sp", y_shift(k)) for k in (1, 2, 3))
    col = jnp.concatenate([a, a1, a2, a3], axis=0)
    row = jnp.concatenate([b, b1, b2, b3, qn], axis=0)
    col1 = lax.ppermute(col, "sp", x_shift(1))
    col3 = lax.ppermute(col, "sp", x_shift(-1))
    row1 = lax.ppermute(row, "sp", y_shift(1))
    row3 = lax.ppermute(row, "sp", y_shift(-1))
    col2l = lax.ppermute(col1[:288], "sp", x_shift(1))
    col2h = lax.ppermute(col3[288:], "sp", x_shift(-1))
    row2l = lax.ppermute(row1[:416], "sp", y_shift(1))
    row2h = lax.ppermute(row3[416:], "sp", y_shift(-1))

    early = expand_early(
        yx, (col, col1, col3, row, row1, row3), w_own, w_other, cosine, sine
    )
    attended = attend(yx, (col2l, col2h, row2l, row2h), cosine, sine, early)
    w_full, *attended = lax.optimization_barrier((w_full, *attended))
    pieces = [attended[0]] + [
        lax.ppermute(attended[i], "sp", y_shift(-i)) for i in range(1, SIDE)
    ]
    mixed = project(y.reshape(1), pieces, stage(w_full), out_gain.reshape(1, 2048))
    return mixed[None]


def solution(mesh):
    in_specs = (
        P("dp", "sp", None),
        P("dp", None),
        P("dp", None),
        P(),
        P(),
        P(),
        P("dp", None),
        P("dp", None),
        P(None, "dp"),
        P(),
    )
    out_specs = P("dp", "sp", None)

    return jax.shard_map(body, mesh=mesh, in_specs=in_specs, out_specs=out_specs, check_vma=False)
```
